256 devices in a mesh: fs: 32 (over z, y), tp: 8 (over x, core).
Axes of the slice: x: 4, y: 4, z: 8, core: 2. Of those that a mesh axis runs over, the one named last changes fastest.
Arguments:
- inputs: bfloat16 [65536, 2048], P('fs'), may hold values from -6 to 6
- cotangents: bfloat16 [3, 65536, 1024], P(None, 'fs', 'tp'), as said below
- factor: bfloat16 [2048, 256], P('fs'), as said below
- weights: float32 [3, 2048, 1024], P(None, 'fs', 'tp'), may hold values from -0.125 to 0.125
- first_moment: float32 [3, 256, 1024], P(None, 'fs', 'tp'), may hold values from -0.6 to 0.6
- second_moment: float32 [3, 256, 1024], P(None, 'fs', 'tp'), may hold values from 0.001 to 0.01
Outputs:
- update: float32 [3, 2048, 1024], P(None, 'fs', 'tp')
- new_weights: float32 [3, 2048, 1024], P(None, 'fs', 'tp')
- copies: bfloat16 [3, 2048, 1024], P(None, None, 'tp')
- new_first: float32 [3, 256, 1024], P(None, 'fs', 'tp')
- new_second: float32 [3, 256, 1024], P(None, 'fs', 'tp')
The draws below stay inside these ranges and needn't reach their ends.
Inputs may be any that keep to these rules, and one draw needn't show every extreme that they name: A real-valued factor of full rank. real-valued cotangents.
All inputs are finite; a program needn't handle non-finite values.
Results may differ from the reference program's by a relative error of at most 0.0085.
Values may be sent and summed in bfloat16 or wider, within the bound.
No kernel may reach another device: no remote copies, remote signals or barrier semaphores. Data moves between devices by JAX's collectives and lax.ppermute only.
A program may use at most 64 MiB of HBM per device.

```python
import math
import jax
import jax.numpy as jnp
from jax import lax

D = 2048
MW = 1024
RANK = 256
TOKENS = 65536


def draw_cotangents(key, part):
    first_key = jax.random.fold_in(jax.random.fold_in(key, 11), 0)
    columns = jnp.arange(MW, dtype=jnp.float32) / max(MW - 1, 1)
    base = jnp.clip(jax.random.normal(first_key, (3, TOKENS, MW), jnp.float32), -6.0, 6.0)
    spread = jnp.power(4.0, columns)
    values = base * spread / TOKENS ** 0.5
    return values.astype(jnp.bfloat16)


def draw_factor(key, part):
    first_key = jax.random.fold_in(key, 23)
    columns = jnp.arange(RANK, dtype=jnp.float32) / max(RANK - 1, 1)
    base = jnp.clip(jax.random.normal(first_key, (D, RANK), jnp.float32), -6.0, 6.0)
    spread = jnp.power(3.0, columns)
    values = base * spread / D ** 0.5
    return values.astype(jnp.bfloat16)


def steps_of(key, extent, cuts, low, high):
    gain, own = 1.0, jax.random.fold_in(key, 6)
    for position, shards_of in cuts:
        heights = jnp.exp(jax.random.uniform(jax.random.fold_in(own, position), (shards_of,), jnp.float32, low / len(cuts), high / len(cuts)))
        gain = gain * jnp.repeat(heights, extent[position] // shards_of).reshape([-1 if axis == position else 1 for axis in range(len(extent))])
    return gain


def bell_draw(own_key, extent, deviation, most, pieces=(), kind=jnp.bfloat16):
    drawn = deviation * jax.random.normal(own_key, extent, jnp.float32)
    if pieces:
        drawn = drawn * steps_of(own_key, extent, pieces, -0.22, 0.18)
    return jnp.clip(drawn, -most, most).astype(kind)


def setup_inputs(seed: int = 0) -> dict:
    key_list = jax.random.split(jax.random.key(seed), 7)
    inputs = bell_draw(key_list[0], (TOKENS, D), 1.0, 6.0, ((0, 32),))
    cotangents = draw_cotangents(jax.random.fold_in(key_list[6], 71), 0)
    factor = draw_factor(jax.random.fold_in(key_list[6], 71), 0)
    weights = bell_draw(key_list[3], (3, D, MW), D ** -0.5, 0.125, ((1, 32), (2, 8)), jnp.float32)
    first_moment = bell_draw(key_list[4], (3, RANK, MW), 0.1, 0.6, ((1, 32), (2, 8)), jnp.float32)
    second_moment = jnp.clip(jnp.exp(math.log(0.01) - 2.30258502 * jax.random.uniform(key_list[5], (3, RANK, MW), jnp.float32) ** steps_of(key_list[5], (3, RANK, MW), ((1, 32), (2, 8)), -0.2, 0.2)), 0.001, 0.01)
    return {"inputs": inputs, "cotangents": cotangents, "factor": factor, "weights": weights, "first_moment": first_moment, "second_moment": second_moment}


def reference(inputs, cotangents, factor, weights, first_moment, second_moment):
    factor_wide = factor.astype(jnp.float32)
    projected_list = []
    for which in range(3):
        gradient = jnp.dot(inputs.T, cotangents[which], preferred_element_type=jnp.float32)
        projected_list.append(jnp.dot(factor_wide.T, gradient, precision=lax.Precision.HIGHEST))
    projected = jnp.stack(projected_list)
    square_sum = jnp.sum(projected * projected)
    root_mean = jnp.sqrt(square_sum / (3 * RANK * MW) + 1e-06)
    clip_factor = jnp.minimum(1.0, 0.25 / root_mean)
    clipped = clip_factor * projected
    new_first = 0.9 * first_moment + 0.1 * clipped
    new_second = 0.95 * second_moment + 0.05 * clipped * clipped
    normed = new_first / (jnp.sqrt(new_second) + 1e-08)
    update = jnp.einsum('dr,mrc->mdc', factor_wide, normed, precision=lax.Precision.HIGHEST)
    new_weights = weights - 0.02 * update
    copies = new_weights.astype(jnp.bfloat16)
    return (update, new_weights, copies, new_first, new_second)
```

```python
import jax
import jax.numpy as jnp
from jax import lax
from jax.sharding import Mesh
from jax.sharding import PartitionSpec as P

MW = 1024
RANK = 256
Z, Y = ("fs_0", "fs_1")
FS = ("fs_0", "fs_1")
TP = ("tp_0", "tp_1")
BF = jnp.bfloat16


def sent_to_all(array, axis):
    copies = jnp.broadcast_to(array, (lax.axis_size(axis), *array.shape))
    return lax.all_to_all(copies, axis, split_axis=0, concat_axis=0, tiled=True)


def staged(array):
    return sent_to_all(sent_to_all(array, Z), Y)


def on_device(inputs, cotangents, factor, weights, first_moment, second_moment):
    with jax.named_scope("factor_gather"):
        factor_all = jnp.transpose(staged(factor), (1, 0, 2, 3)).reshape(-1, RANK)
    with jax.named_scope("gradient"):
        local_gradient = jnp.einsum(
            "td,mtc->dmc", inputs, cotangents, preferred_element_type=jnp.float32
        )
        gradient_high = local_gradient.astype(BF)
        gradient_low = (local_gradient - gradient_high.astype(jnp.float32)).astype(BF)
    with jax.named_scope("state_gather"):
        state = jnp.concatenate([weights, first_moment, second_moment], axis=1).astype(BF)
        state_all = jnp.transpose(staged(state), (2, 1, 0, 3, 4))
        weights_all = state_all[:, :, :, :64].reshape(3, -1, 128).astype(jnp.float32)
        first_all = state_all[:, :, :, 64:72].reshape(3, -1, 128).astype(jnp.float32)
        second_all = state_all[:, :, :, 72:].reshape(3, -1, 128).astype(jnp.float32)
    with jax.named_scope("partial"):
        high_term = jnp.einsum(
            "dr,dmc->rmc", factor_all, gradient_high, preferred_element_type=jnp.float32
        )
        low_term = jnp.einsum(
            "dr,dmc->rmc", factor_all, gradient_low, preferred_element_type=jnp.float32
        )
        partial_value = (high_term + low_term).astype(BF).reshape(32, 8, 3, 128)
    with jax.named_scope("partial_exchange"):
        arrived = lax.all_to_all(partial_value, FS, split_axis=0, concat_axis=0, tiled=True)
        projected = jnp.transpose(arrived.astype(jnp.float32).sum(axis=0), (1, 0, 2))
    with jax.named_scope("projected_gather"):
        projected_all = sent_to_all(projected.astype(BF), FS)
        projected_all = (
            jnp.transpose(projected_all, (1, 0, 2, 3)).reshape(3, -1, 128).astype(jnp.float32)
        )
    with jax.named_scope("square_sum"):
        square_sum = jnp.sum(projected_all * projected_all)
        square_sum = jnp.sum(sent_to_all(jnp.full((1, 128), square_sum), TP)[:, 0, 0])
        root_mean = jnp.sqrt(square_sum / (3 * RANK * MW) + 1e-06)
        clip_factor = jnp.minimum(1.0, 0.25 / root_mean)

    def moments(projected, first_moment, second_moment):
        clipped = clip_factor * projected
        new_first = 0.9 * first_moment + 0.1 * clipped
        new_second = 0.95 * second_moment + 0.05 * clipped * clipped
        return new_first, new_second, new_first / (jnp.sqrt(new_second) + 1e-08)

    with jax.named_scope("own_moments"):
        new_first, new_second, _ = moments(projected, first_moment, second_moment)
    with jax.named_scope("update"):
        normed = moments(projected_all, first_all, second_all)[2].astype(BF)
        update = jnp.einsum("dr,mrc->mdc", factor, normed, preferred_element_type=jnp.float32)
        new_weights = weights - 0.02 * update
        update_all = jnp.einsum(
            "dr,mrc->mdc", factor_all, normed, preferred_element_type=jnp.float32
        )
        copies = (weights_all - 0.02 * update_all).astype(BF)
    return (update, new_weights, copies, new_first, new_second)


def solution(mesh):
    torus = Mesh(mesh.devices.reshape(8, 4, 4, 2), ("fs_0", "fs_1", "tp_0", "tp_1"))
    return jax.shard_map(
        on_device,
        mesh=torus,
        in_specs=(
            P(FS, None),
            P(None, FS, TP),
            P(FS, None),
            P(None, FS, TP),
            P(None, FS, TP),
            P(None, FS, TP),
        ),
        out_specs=(
            P(None, FS, TP),
            P(None, FS, TP),
            P(None, None, TP),
            P(None, FS, TP),
            P(None, FS, TP),
        ),
        check_vma=False,
    )
```

```python
import jax
import jax.numpy as jnp
from jax import lax
from jax.experimental import pallas as pl
from jax.experimental.pallas import tpu as pltpu
from jax.sharding import Mesh
from jax.sharding import PartitionSpec as P

MW = 1024
RANK = 256
Z, Y = ("fs_0", "fs_1")
FS = ("fs_0", "fs_1")
TP = ("tp_0", "tp_1")
CORE = "tp_1"
BF = jnp.bfloat16
F32 = jnp.float32
VMEM = pl.BlockSpec(memory_space=pltpu.VMEM)


def sent_to_all(array, axis):
    copies = jnp.broadcast_to(array, (lax.axis_size(axis), *array.shape))
    return lax.all_to_all(copies, axis, split_axis=0, concat_axis=0, tiled=True)


def moved(array, axis, shift):
    size = lax.axis_size(axis)
    return lax.ppermute(array, axis, [(i, (i + shift) % size) for i in range(size)])


def gathered_z(array):
    right, left = [array], [array]
    for _ in range(3):
        right.append(moved(right[-1], Z, 1))
        left.append(moved(left[-1], Z, -1))
    right.append(moved(right[-1], Z, 1))
    return jnp.stack(right + left[:0:-1])


def gathered_y(array):
    right = moved(array, Y, 1)
    left = moved(array, Y, -1)
    return (
        array, right, left,
        moved(right[:4], Y, 1), moved(left[4:], Y, -1),
    )


def partial_kernel(core, gradient_a, gradient_b, mine, other, out, factor):
    for z in range(8):
        for y in range(4):
            row = z * 256 + y * 64
            factor[pl.ds(row + pl.multiple_of(core[0] * 32, 32), 32)] = mine[y, z]
            factor[pl.ds(row + pl.multiple_of(32 - core[0] * 32, 32), 32)] = other[y, z]
    projected = jnp.dot(gradient_a[...], factor[:1024], preferred_element_type=F32)
    projected += jnp.dot(gradient_b[...], factor[1024:], preferred_element_type=F32)
    rows = [projected[m * 128 : (m + 1) * 128].T.reshape(32, 8, 128) for m in range(3)]
    out[...] = jnp.concatenate(rows, axis=1).astype(BF)


def square_kernel(projected, out):
    values = projected[...].astype(F32).reshape(96, 8, 128)
    out[...] = jnp.broadcast_to(jnp.sum(values * values, axis=0), out.shape)


def moments(clip, projected, first, second):
    clipped = clip * projected
    new_first = 0.9 * first + 0.1 * clipped
    new_second = 0.95 * second + 0.05 * clipped * clipped
    return new_first, new_second, new_first / (jnp.sqrt(new_second) + 1e-08)


def final_kernel(
    place, squares, projected, own, state, right, left, across_a, across_b,
    first, second, weights, factor, own_factor,
    update, new_weights, copies, new_first, new_second, normed, change,
):
    total = jnp.sum(jnp.sum(squares[...], axis=0), keepdims=True)
    root_mean = jnp.sqrt(total / (3 * RANK * MW) + 1e-06)
    clip = jnp.minimum(1.0, 0.25 / root_mean)
    blocks = []
    for j in range(8):
        across = across_a.at[j] if j < 4 else across_b.at[j - 4]
        for i, block in enumerate((state.at[j], right.at[j], across, left.at[j])):
            at = ((place[0] + 8 - j) % 8) * 4 + (place[1] + 4 - i) % 4
            blocks.append((at, block))
    for at, block in blocks:
        _, _, values = moments(
            clip,
            projected[at].astype(F32),
            block[192:216].astype(F32),
            block[216:240].astype(F32),
        )
        for m in range(3):
            normed[pl.ds(pl.multiple_of(at * 8, 8), 8), m * 128 : (m + 1) * 128] = values[
                m * 8 : (m + 1) * 8
            ]
    values = normed[...].astype(BF)
    own_change = jnp.dot(own_factor[...], values, preferred_element_type=F32)
    for m in range(3):
        part = own_change[:, m * 128 : (m + 1) * 128]
        update[m] = part
        new_weights[m] = weights[m] - 0.02 * part
        own_first, own_second, _ = moments(
            clip, own[m * 8 : (m + 1) * 8], first[m], second[m]
        )
        new_first[m] = own_first
        new_second[m] = own_second
    change[...] = jnp.dot(factor[...], values, preferred_element_type=F32)
    for at, block in blocks:
        rows = pl.ds(pl.multiple_of(at * 64, 64), 64)
        for m in range(3):
            before = block[m * 64 : (m + 1) * 64].astype(F32)
            part = change[rows, m * 128 : (m + 1) * 128]
            copies[m, rows] = (before - 0.02 * part).astype(BF)


def step(inputs, cotangents, factor, weights, first_moment, second_moment):
    core = lax.axis_index(CORE)
    place = jnp.stack([lax.axis_index(Z), lax.axis_index(Y)]).astype(jnp.int32)
    half = lax.dynamic_slice_in_dim(factor, core * 32, 32, 0)
    half = sent_to_all(half, Z)
    half = sent_to_all(half, Y)
    other_half = moved(half, CORE, 1)
    state = jnp.concatenate(
        [array.reshape(-1, 128) for array in (weights, first_moment, second_moment)]
    ).astype(BF)
    state_z = gathered_z(state)
    states = gathered_y(state_z)

    def gradient_of(part):
        return (
            jnp.einsum("mtc,td->mcd", cotangents, part, preferred_element_type=F32)
            .astype(BF)
            .reshape(384, -1)
        )

    gradient_a = gradient_of(inputs[:, :1024])
    gradient_b = gradient_of(inputs[:, 1024:])
    smem = pl.BlockSpec(memory_space=pltpu.SMEM)
    partial_value, factor_all = pl.pallas_call(
        partial_kernel,
        out_shape=(
            jax.ShapeDtypeStruct((32, 24, 128), BF),
            jax.ShapeDtypeStruct((2048, RANK), BF),
        ),
        in_specs=[smem] + [VMEM] * 4,
        out_specs=(VMEM, VMEM),
        compiler_params=pltpu.CompilerParams(vmem_limit_bytes=12 << 20),
    )(core.reshape(1).astype(jnp.int32), gradient_a, gradient_b, half, other_half)
    arrived = lax.all_to_all(partial_value, FS, split_axis=0, concat_axis=0, tiled=True)
    projected = arrived.astype(F32).sum(axis=0)
    projected_all = sent_to_all(projected.astype(BF), FS)
    squares = pl.pallas_call(
        square_kernel,
        out_shape=jax.ShapeDtypeStruct((8, 8, 128), F32),
        in_specs=[VMEM],
        out_specs=VMEM,
        compiler_params=pltpu.CompilerParams(vmem_limit_bytes=4 << 20),
    )(projected_all)
    squares = lax.all_to_all(squares, TP, split_axis=0, concat_axis=0, tiled=True)
    return pl.pallas_call(
        final_kernel,
        out_shape=(
            jax.ShapeDtypeStruct((3, 64, 128), F32),
            jax.ShapeDtypeStruct((3, 64, 128), F32),
            jax.ShapeDtypeStruct((3, 2048, 128), BF),
            jax.ShapeDtypeStruct((3, 8, 128), F32),
            jax.ShapeDtypeStruct((3, 8, 128), F32),
        ),
        in_specs=[smem] + [VMEM] * 13,
        out_specs=(VMEM,) * 5,
        scratch_shapes=[pltpu.VMEM((RANK, 384), F32), pltpu.VMEM((2048, 384), F32)],
        compiler_params=pltpu.CompilerParams(vmem_limit_bytes=24 << 20),
    )(
        place, squares, projected_all, projected, *states, first_moment, second_moment,
        weights, factor_all, factor,
    )


def solution(mesh):
    torus = Mesh(mesh.devices.reshape(8, 4, 4, 2), ("fs_0", "fs_1", "tp_0", "tp_1"))
    return jax.shard_map(
        step,
        mesh=torus,
        in_specs=(
            P(FS, None),
            P(None, FS, TP),
            P(FS, None),
            P(None, FS, TP),
            P(None, FS, TP),
            P(None, FS, TP),
        ),
        out_specs=(
            P(None, FS, TP),
            P(None, FS, TP),
            P(None, None, TP),
            P(None, FS, TP),
            P(None, FS, TP),
        ),
        check_vma=False,
    )
```

```python
import jax
import jax.numpy as jnp
from jax import lax
from jax.experimental import pallas as pl
from jax.experimental.pallas import tpu as pltpu
from jax.sharding import Mesh
from jax.sharding import PartitionSpec as P

MW = 1024
RANK = 256
Z, Y = ("fs_0", "fs_1")
FS = ("fs_0", "fs_1")
TP = ("tp_0", "tp_1")
CORE = "tp_1"
BF = jnp.bfloat16
F32 = jnp.float32
VMEM = pl.BlockSpec(memory_space=pltpu.VMEM)


def sent_to_all(array, axis):
    copies = jnp.broadcast_to(array, (lax.axis_size(axis), *array.shape))
    return lax.all_to_all(copies, axis, split_axis=0, concat_axis=0, tiled=True)


def moved(array, axis, shift):
    size = lax.axis_size(axis)
    return lax.ppermute(array, axis, [(i, (i + shift) % size) for i in range(size)])


def swapped(array, axis, bit):
    size = lax.axis_size(axis)
    return lax.ppermute(array, axis, [(i, i ^ bit) for i in range(size)])


def gathered_z(array):
    array = array[None]
    for bit in (4, 2, 1):
        array = jnp.concatenate([array, swapped(array, Z, bit)])
    return array


def gathered_y(array):
    right = moved(array, Y, 1)
    left = moved(array, Y, -1)
    return (
        array, right, left,
        moved(right[:4], Y, 1), moved(left[4:], Y, -1),
    )


def gradient_kernel(cotangents, inputs, out, turned):
    @pl.when(pl.program_id(0) == 0)
    def _():
        for m in range(3):
            turned[m * 128 : (m + 1) * 128] = cotangents[m].T

    out[...] = jnp.dot(turned[...], inputs[...], preferred_element_type=F32).astype(BF)


def assemble(core, mine, other, factor):
    for z in range(8):
        for y in range(4):
            row = z * 256 + y * 64
            factor[pl.ds(row + pl.multiple_of(core[0] * 32, 32), 32)] = mine[y, z]
            factor[pl.ds(row + pl.multiple_of(32 - core[0] * 32, 32), 32)] = other[y, z]


def partial_kernel(core, gradient, mine, other, out, factor):
    assemble(core, mine, other, factor)
    projected = jnp.dot(gradient[...], factor[...], preferred_element_type=F32)
    rows = [projected[m * 128 : (m + 1) * 128].T.reshape(32, 8, 128) for m in range(3)]
    out[...] = jnp.concatenate(rows, axis=1).astype(BF)


def square_kernel(projected, out):
    values = projected[...].astype(F32).reshape(96, 8, 128)
    out[...] = jnp.broadcast_to(jnp.sum(values * values, axis=0), out.shape)


def moments(clip, projected, first, second):
    clipped = clip * projected
    new_first = 0.9 * first + 0.1 * clipped
    new_second = 0.95 * second + 0.05 * clipped * clipped
    return new_first, new_second, new_first / (jnp.sqrt(new_second) + 1e-08)


def final_kernel(
    place, squares, projected, own, state, right, left, across_a, across_b,
    first, second, weights, factor, own_factor,
    update, new_weights, copies, new_first, new_second, normed, change,
):
    total = jnp.sum(jnp.sum(squares[...], axis=0), keepdims=True)
    root_mean = jnp.sqrt(total / (3 * RANK * MW) + 1e-06)
    clip = jnp.minimum(1.0, 0.25 / root_mean)
    blocks = []
    for j in range(8):
        across = across_a.at[j] if j < 4 else across_b.at[j - 4]
        for i, block in enumerate((state.at[j], right.at[j], across, left.at[j])):
            away = j // 4 + (j // 2 % 2) * 2 + (j % 2) * 4
            at = (place[0] ^ away) * 4 + (place[1] + 4 - i) % 4
            blocks.append((at, block))
    for at, block in blocks:
        _, _, values = moments(
            clip,
            projected[at].astype(F32),
            block[192:216].astype(F32),
            block[216:240].astype(F32),
        )
        for m in range(3):
            normed[pl.ds(pl.multiple_of(at * 8, 8), 8), m * 128 : (m + 1) * 128] = values[
                m * 8 : (m + 1) * 8
            ]
    values = normed[...].astype(BF)
    own_change = jnp.dot(own_factor[...], values, preferred_element_type=F32)
    for m in range(3):
        part = own_change[:, m * 128 : (m + 1) * 128]
        update[m] = part
        new_weights[m] = weights[m] - 0.02 * part
        own_first, own_second, _ = moments(
            clip, own[m * 8 : (m + 1) * 8], first[m], second[m]
        )
        new_first[m] = own_first
        new_second[m] = own_second
    change[...] = jnp.dot(factor[...], values, preferred_element_type=F32)
    for at, block in blocks:
        rows = pl.ds(pl.multiple_of(at * 64, 64), 64)
        for m in range(3):
            before = block[m * 64 : (m + 1) * 64].astype(F32)
            part = change[rows, m * 128 : (m + 1) * 128]
            copies[m, rows] = (before - 0.02 * part).astype(BF)


def step(inputs, cotangents, factor, weights, first_moment, second_moment):
    core = lax.axis_index(CORE)
    place = jnp.stack([lax.axis_index(Z), lax.axis_index(Y)]).astype(jnp.int32)
    half = lax.dynamic_slice_in_dim(factor, core * 32, 32, 0)
    half = sent_to_all(half, Z)
    half = sent_to_all(half, Y)
    other_half = moved(half, CORE, 1)
    state = jnp.concatenate(
        [array.reshape(-1, 128) for array in (weights, first_moment, second_moment)]
    ).astype(BF)
    state_z = gathered_z(state)
    states = gathered_y(state_z)

    gradient = pl.pallas_call(
        gradient_kernel,
        grid=(8,),
        out_shape=jax.ShapeDtypeStruct((384, 2048), BF),
        in_specs=[
            pl.BlockSpec((3, 2048, 128), lambda n: (0, 0, 0)),
            pl.BlockSpec((2048, 256), lambda n: (0, n)),
        ],
        out_specs=pl.BlockSpec((384, 256), lambda n: (0, n)),
        scratch_shapes=[pltpu.VMEM((384, 2048), BF)],
        compiler_params=pltpu.CompilerParams(vmem_limit_bytes=57 << 20),
    )(cotangents, inputs)
    smem = pl.BlockSpec(memory_space=pltpu.SMEM)
    core_id = core.reshape(1).astype(jnp.int32)
    partial_value = pl.pallas_call(
        partial_kernel,
        out_shape=jax.ShapeDtypeStruct((32, 24, 128), BF),
        in_specs=[smem] + [VMEM] * 3,
        out_specs=VMEM,
        scratch_shapes=[pltpu.VMEM((2048, RANK), BF)],
        compiler_params=pltpu.CompilerParams(vmem_limit_bytes=12 << 20),
    )(core_id, gradient, half, other_half)
    factor_all = pl.pallas_call(
        assemble,
        out_shape=jax.ShapeDtypeStruct((2048, RANK), BF),
        in_specs=[smem] + [VMEM] * 2,
        out_specs=VMEM,
        compiler_params=pltpu.CompilerParams(vmem_limit_bytes=8 << 20),
    )(core_id, half, other_half)
    arrived = lax.all_to_all(partial_value, FS, split_axis=0, concat_axis=0, tiled=True)
    projected = arrived.astype(F32).sum(axis=0)
    projected_all = sent_to_all(projected.astype(BF), FS)
    squares = pl.pallas_call(
        square_kernel,
        out_shape=jax.ShapeDtypeStruct((8, 8, 128), F32),
        in_specs=[VMEM],
        out_specs=VMEM,
        compiler_params=pltpu.CompilerParams(vmem_limit_bytes=4 << 20),
    )(projected_all)
    squares = lax.all_to_all(squares, TP, split_axis=0, concat_axis=0, tiled=True)
    return pl.pallas_call(
        final_kernel,
        out_shape=(
            jax.ShapeDtypeStruct((3, 64, 128), F32),
            jax.ShapeDtypeStruct((3, 64, 128), F32),
            jax.ShapeDtypeStruct((3, 2048, 128), BF),
            jax.ShapeDtypeStruct((3, 8, 128), F32),
            jax.ShapeDtypeStruct((3, 8, 128), F32),
        ),
        in_specs=[smem] + [VMEM] * 13,
        out_specs=(VMEM,) * 5,
        scratch_shapes=[pltpu.VMEM((RANK, 384), F32), pltpu.VMEM((2048, 384), F32)],
        compiler_params=pltpu.CompilerParams(vmem_limit_bytes=24 << 20),
    )(
        place, squares, projected_all, projected, *states, first_moment, second_moment,
        weights, factor_all, factor,
    )


def solution(mesh):
    torus = Mesh(mesh.devices.reshape(8, 4, 4, 2), ("fs_0", "fs_1", "tp_0", "tp_1"))
    return jax.shard_map(
        step,
        mesh=torus,
        in_specs=(
            P(FS, None),
            P(None, FS, TP),
            P(FS, None),
            P(None, FS, TP),
            P(None, FS, TP),
            P(None, FS, TP),
        ),
        out_specs=(
            P(None, FS, TP),
            P(None, FS, TP),
            P(None, None, TP),
            P(None, FS, TP),
            P(None, FS, TP),
        ),
        check_vma=False,
    )
```

```python
import jax
import jax.numpy as jnp
from jax import lax
from jax.experimental import pallas as pl
from jax.experimental.pallas import tpu as pltpu
from jax.sharding import Mesh
from jax.sharding import PartitionSpec as P

MW = 1024
RANK = 256
Z, Y = ("fs_0", "fs_1")
FS = ("fs_0", "fs_1")
TP = ("tp_0", "tp_1")
CORE = "tp_1"
BF = jnp.bfloat16
F32 = jnp.float32
VMEM = pl.BlockSpec(memory_space=pltpu.VMEM)


def sent_to_all(array, axis):
    copies = jnp.broadcast_to(array, (lax.axis_size(axis), *array.shape))
    return lax.all_to_all(copies, axis, split_axis=0, concat_axis=0, tiled=True)


def moved(array, axis, shift):
    size = lax.axis_size(axis)
    return lax.ppermute(array, axis, [(i, (i + shift) % size) for i in range(size)])


def swapped(array, axis, bit):
    size = lax.axis_size(axis)
    return lax.ppermute(array, axis, [(i, i ^ bit) for i in range(size)])


def gathered_z(array):
    for bit in (4, 2, 1):
        array = jnp.concatenate([array, swapped(array, Z, bit)])
    return array


def gathered_y(array):
    right = moved(array, Y, 1)
    left = moved(array, Y, -1)
    return (
        array, right, left,
        moved(right[:4], Y, 1), moved(left[4:], Y, -1),
    )


def spread_kernel(place, factor, out):
    rows = factor[pl.ds(pl.multiple_of(place[2] * 32, 32), 32)]
    out[...] = jnp.broadcast_to(rows, out.shape)


def state_kernel(weights, first, second, out):
    out[0, :192] = weights[...].reshape(192, 128).astype(BF)
    moments = jnp.concatenate([first[...].reshape(24, 128), second[...].reshape(24, 128)])
    out[0, 192:] = moments.astype(BF)


def assemble(place, mine, other, factor):
    for z in range(8):
        for y in range(4):
            row = z * 256 + y * 64
            factor[pl.ds(row + pl.multiple_of(place[2] * 32, 32), 32)] = mine[y, z]
            factor[pl.ds(row + pl.multiple_of(32 - place[2] * 32, 32), 32)] = other[y, z]


def partial_kernel(place, gradient_a, gradient_b, mine, other, out, factor, held, sem):
    copy = pltpu.make_async_copy(gradient_b, held, sem)
    copy.start()
    assemble(place, mine, other, factor)
    projected = jnp.dot(gradient_a[...], factor[:1024], preferred_element_type=F32)
    copy.wait()
    projected += jnp.dot(held[...], factor[1024:], preferred_element_type=F32)
    rows = [projected[m * 128 : (m + 1) * 128].T.reshape(32, 8, 128) for m in range(3)]
    out[...] = jnp.concatenate(rows, axis=1).astype(BF)


def square_kernel(projected, out):
    values = projected[...].astype(F32).reshape(96, 8, 128)
    out[...] = jnp.broadcast_to(jnp.sum(values * values, axis=0), out.shape)


def moments(clip, projected, first, second):
    clipped = clip * projected
    new_first = 0.9 * first + 0.1 * clipped
    new_second = 0.95 * second + 0.05 * clipped * clipped
    return new_first, new_second, new_first / (jnp.sqrt(new_second) + 1e-08)


def final_kernel(
    place, squares, projected, own, state, right, left, across_a, across_b,
    first, second, weights, factor, own_factor,
    update_out, weights_out, copies_out, first_out, second_out,
    update, new_weights, copies, new_first, new_second, normed, change, own_sems, sems,
):
    total = jnp.sum(jnp.sum(squares[...], axis=0), keepdims=True)
    root_mean = jnp.sqrt(total / (3 * RANK * MW) + 1e-06)
    clip = jnp.minimum(1.0, 0.25 / root_mean)

    def blocks_of(j):
        across = across_a.at[j] if j < 4 else across_b.at[j - 4]
        z = place[0] ^ (j // 4 + (j // 2 % 2) * 2 + (j % 2) * 4)
        return [
            (z * 4 + (place[1] + 4 - i) % 4, block)
            for i, block in enumerate((state.at[j], right.at[j], across, left.at[j]))
        ]

    blocks = [blocks_of(j) for j in range(8)]
    for m in range(3):
        own_first, own_second, _ = moments(
            clip, own[m * 8 : (m + 1) * 8], first[m], second[m]
        )
        new_first[m] = own_first
        new_second[m] = own_second
    for j in range(8):
        for at, block in blocks[j]:
            _, _, values = moments(
                clip,
                projected[at].astype(F32),
                block[192:216].astype(F32),
                block[216:240].astype(F32),
            )
            for m in range(3):
                normed[pl.ds(pl.multiple_of(at * 8, 8), 8), m * 128 : (m + 1) * 128] = values[
                    m * 8 : (m + 1) * 8
                ]
    values = normed[...].astype(BF)
    own_change = jnp.dot(own_factor[...], values, preferred_element_type=F32)
    for m in range(3):
        part = own_change[:, m * 128 : (m + 1) * 128]
        update[m] = part
        new_weights[m] = weights[m] - 0.02 * part
    sent = [
        pltpu.make_async_copy(source, target, own_sems.at[k])
        for k, (source, target) in enumerate(
            (
                (update, update_out), (new_weights, weights_out),
                (new_first, first_out), (new_second, second_out),
            )
        )
    ]
    for copy in sent:
        copy.start()
    for q in range(4):
        base = pl.multiple_of(blocks[q][0][0] // 8 * 512, 512)
        change[q % 2] = jnp.dot(
            factor[pl.ds(base, 512)], values, preferred_element_type=F32
        )
        for at, block in blocks[q] + blocks[q + 4]:
            rows = pl.ds(pl.multiple_of(at * 64, 64), 64)
            inner = pl.ds(pl.multiple_of(at * 64 - base, 64), 64)
            for m in range(3):
                before = block[m * 64 : (m + 1) * 64].astype(F32)
                part = change[q % 2, inner, m * 128 : (m + 1) * 128]
                copies[m, rows] = (before - 0.02 * part).astype(BF)
        for m in range(3):
            rows = pl.ds(base, 512)
            copy = pltpu.make_async_copy(
                copies.at[m, rows], copies_out.at[m, rows], sems.at[q, m]
            )
            copy.start()
            sent.append(copy)
    for copy in sent:
        copy.wait()


def step(inputs, cotangents, factor, weights, first_moment, second_moment):
    place = jnp.stack([lax.axis_index(axis) for axis in (Z, Y, CORE)]).astype(jnp.int32)
    smem = pl.BlockSpec(memory_space=pltpu.SMEM)
    hbm = pl.BlockSpec(memory_space=pl.ANY)
    half = pl.pallas_call(
        spread_kernel,
        out_shape=jax.ShapeDtypeStruct((8, 32, RANK), BF),
        in_specs=[smem, VMEM],
        out_specs=VMEM,
        compiler_params=pltpu.CompilerParams(vmem_limit_bytes=60 << 20),
    )(place, factor)
    half = lax.all_to_all(half, Z, split_axis=0, concat_axis=0, tiled=True)
    half = sent_to_all(half, Y)
    other_half = moved(half, CORE, 1)
    state = pl.pallas_call(
        state_kernel,
        out_shape=jax.ShapeDtypeStruct((1, 240, 128), BF),
        in_specs=[VMEM] * 3,
        out_specs=VMEM,
        compiler_params=pltpu.CompilerParams(vmem_limit_bytes=60 << 20),
    )(weights, first_moment, second_moment)
    state_z = gathered_z(state)
    states = gathered_y(state_z)


    def gradient_of(part):
        return (
            jnp.einsum("mtc,td->mcd", cotangents, part, preferred_element_type=F32)
            .astype(BF)
            .reshape(384, -1)
        )

    gradient_a = gradient_of(inputs[:, :1024])
    gradient_b = gradient_of(inputs[:, 1024:])
    partial_value = pl.pallas_call(
        partial_kernel,
        out_shape=jax.ShapeDtypeStruct((32, 24, 128), BF),
        in_specs=[smem, VMEM, hbm, VMEM, VMEM],
        out_specs=VMEM,
        scratch_shapes=[
            pltpu.VMEM((2048, RANK), BF),
            pltpu.VMEM((384, 1024), BF),
            pltpu.SemaphoreType.DMA,
        ],
        compiler_params=pltpu.CompilerParams(vmem_limit_bytes=12 << 20),
    )(place, gradient_a, gradient_b, half, other_half)
    factor_all = pl.pallas_call(
        assemble,
        out_shape=jax.ShapeDtypeStruct((2048, RANK), BF),
        in_specs=[smem] + [VMEM] * 2,
        out_specs=VMEM,
        compiler_params=pltpu.CompilerParams(vmem_limit_bytes=8 << 20),
    )(place, half, other_half)
    arrived = lax.all_to_all(partial_value, FS, split_axis=0, concat_axis=0, tiled=True)
    projected = arrived.astype(F32).sum(axis=0)
    projected_all = sent_to_all(projected.astype(BF), FS)
    squares = pl.pallas_call(
        square_kernel,
        out_shape=jax.ShapeDtypeStruct((8, 8, 128), F32),
        in_specs=[VMEM],
        out_specs=VMEM,
        compiler_params=pltpu.CompilerParams(vmem_limit_bytes=4 << 20),
    )(projected_all)
    squares = lax.all_to_all(squares, TP, split_axis=0, concat_axis=0, tiled=True)
    return pl.pallas_call(
        final_kernel,
        out_shape=(
            jax.ShapeDtypeStruct((3, 64, 128), F32),
            jax.ShapeDtypeStruct((3, 64, 128), F32),
            jax.ShapeDtypeStruct((3, 2048, 128), BF),
            jax.ShapeDtypeStruct((3, 8, 128), F32),
            jax.ShapeDtypeStruct((3, 8, 128), F32),
        ),
        in_specs=[smem] + [VMEM] * 13,
        out_specs=(hbm,) * 5,
        scratch_shapes=[
            pltpu.VMEM((3, 64, 128), F32),
            pltpu.VMEM((3, 64, 128), F32),
            pltpu.VMEM((3, 2048, 128), BF),
            pltpu.VMEM((3, 8, 128), F32),
            pltpu.VMEM((3, 8, 128), F32),
            pltpu.VMEM((RANK, 384), F32),
            pltpu.VMEM((2, 512, 384), F32),
            pltpu.SemaphoreType.DMA((4,)),
            pltpu.SemaphoreType.DMA((4, 3)),
        ],
        compiler_params=pltpu.CompilerParams(vmem_limit_bytes=24 << 20),
    )(
        place, squares, projected_all, projected, *states, first_moment, second_moment,
        weights, factor_all, factor,
    )


def solution(mesh):
    torus = Mesh(mesh.devices.reshape(8, 4, 4, 2), ("fs_0", "fs_1", "tp_0", "tp_1"))
    return jax.shard_map(
        step,
        mesh=torus,
        in_specs=(
            P(FS, None),
            P(None, FS, TP),
            P(FS, None),
            P(None, FS, TP),
            P(None, FS, TP),
            P(None, FS, TP),
        ),
        out_specs=(
            P(None, FS, TP),
            P(None, FS, TP),
            P(None, None, TP),
            P(None, FS, TP),
            P(None, FS, TP),
        ),
        check_vma=False,
    )
```

```python
import jax
import jax.numpy as jnp
from jax import lax
from jax.experimental import pallas as pl
from jax.experimental.pallas import tpu as pltpu
from jax.sharding import Mesh
from jax.sharding import PartitionSpec as P

MW = 1024
RANK = 256
Z, Y = ("fs_0", "fs_1")
FS = ("fs_0", "fs_1")
TP = ("tp_0", "tp_1")
CORE = "tp_1"
AWAY = (0, 7, 6, 5, 2, 1, 4, 3)
CUT = 1024
BF = jnp.bfloat16
F32 = jnp.float32
VMEM = pl.BlockSpec(memory_space=pltpu.VMEM)


def sent_to_all(array, axis):
    copies = jnp.broadcast_to(array, (lax.axis_size(axis), *array.shape))
    return lax.all_to_all(copies, axis, split_axis=0, concat_axis=0, tiled=True)


def moved(array, axis, shift):
    size = lax.axis_size(axis)
    return lax.ppermute(array, axis, [(i, (i + shift) % size) for i in range(size)])


def gathered_z(array):
    pair = jnp.concatenate([array, moved(array, Z, 1)])
    below = moved(pair, Z, 2)
    above = moved(pair, Z, -2)
    return jnp.concatenate([pair, below, above, moved(above, Z, -2)])


def gathered_y(array):
    right = moved(array, Y, 1)
    left = moved(array, Y, -1)
    return (
        array, right, left,
        moved(right[:4], Y, 1), moved(left[4:], Y, -1),
    )


def spread_kernel(place, factor, out):
    rows = factor[pl.ds(pl.multiple_of(place[2] * 32, 32), 32)]
    out[...] = jnp.broadcast_to(rows, out.shape)


def state_kernel(weights, first, second, out):
    out[0, :192] = weights[...].reshape(192, 128).astype(BF)
    moments = jnp.concatenate([first[...].reshape(24, 128), second[...].reshape(24, 128)])
    out[0, 192:] = moments.astype(BF)


def partial_kernel(
    place, gradient, cotangents, inputs, mine, other,
    out, factor_out, factor, held, seen, turned, mapped, sems, factor_sem,
):
    copies = [
        pltpu.make_async_copy(
            inputs.at[pl.ds(n * 512, 512), pl.ds(CUT, 2048 - CUT)], held.at[n], sems.at[n]
        )
        for n in range(4)
    ]
    copies += [
        pltpu.make_async_copy(cotangents.at[m], seen.at[m], sems.at[4 + m]) for m in range(3)
    ]
    for copy in copies[4:] + copies[:4]:
        copy.start()
    for z in range(8):
        for y in range(4):
            row = z * 256 + y * 64
            factor[pl.ds(row + pl.multiple_of(place[2] * 32, 32), 32)] = mine[y, z]
            factor[pl.ds(row + pl.multiple_of(32 - place[2] * 32, 32), 32)] = other[y, z]
    factor_copy = pltpu.make_async_copy(factor, factor_out, factor_sem)
    factor_copy.start()
    projected = jnp.dot(gradient[...], factor[:CUT], preferred_element_type=F32)
    for m in range(3):
        copies[4 + m].wait()
        turned[m * 128 : (m + 1) * 128] = seen[m].T
    for n in range(4):
        copies[n].wait()
        mapped[n * 512 : (n + 1) * 512] = jnp.dot(
            held[n], factor[CUT:], preferred_element_type=F32
        ).astype(BF)
    projected += jnp.dot(turned[...], mapped[...], preferred_element_type=F32)
    rows = [projected[m * 128 : (m + 1) * 128].T.reshape(32, 8, 128) for m in range(3)]
    out[...] = jnp.concatenate(rows, axis=1).astype(BF)
    factor_copy.wait()


def square_kernel(projected, out):
    values = projected[...].astype(F32).reshape(96, 8, 128)
    out[...] = jnp.broadcast_to(jnp.sum(values * values, axis=0), out.shape)


def moments(clip, projected, first, second):
    clipped = clip * projected
    new_first = 0.9 * first + 0.1 * clipped
    new_second = 0.95 * second + 0.05 * clipped * clipped
    return new_first, new_second, new_first / (jnp.sqrt(new_second) + 1e-08)


def final_kernel(
    place, squares, projected, own, state, right, left, across_a, across_b,
    first, second, weights, factor, own_factor,
    update_out, weights_out, copies_out, first_out, second_out,
    update, new_weights, copies, new_first, new_second, normed, change, own_sems, sems,
):
    total = jnp.sum(jnp.sum(squares[...], axis=0), keepdims=True)
    root_mean = jnp.sqrt(total / (3 * RANK * MW) + 1e-06)
    clip = jnp.minimum(1.0, 0.25 / root_mean)

    def blocks_of(j):
        across = across_a.at[j] if j < 4 else across_b.at[j - 4]
        z = (place[0] + AWAY[j]) % 8
        return [
            (z * 4 + (place[1] + 4 - i) % 4, block)
            for i, block in enumerate((state.at[j], right.at[j], across, left.at[j]))
        ]

    blocks = [blocks_of(j) for j in range(8)]
    for m in range(3):
        own_first, own_second, _ = moments(
            clip, own[m * 8 : (m + 1) * 8], first[m], second[m]
        )
        new_first[m] = own_first
        new_second[m] = own_second
    for j in range(8):
        for at, block in blocks[j]:
            _, _, values = moments(
                clip,
                projected[at].astype(F32),
                block[192:216].astype(F32),
                block[216:240].astype(F32),
            )
            for m in range(3):
                normed[pl.ds(pl.multiple_of(at * 8, 8), 8), m * 128 : (m + 1) * 128] = values[
                    m * 8 : (m + 1) * 8
                ]
    values = normed[...].astype(BF)
    own_change = jnp.dot(own_factor[...], values, preferred_element_type=F32)
    for m in range(3):
        part = own_change[:, m * 128 : (m + 1) * 128]
        update[m] = part
        new_weights[m] = weights[m] - 0.02 * part
    sent = [
        pltpu.make_async_copy(source, target, own_sems.at[k])
        for k, (source, target) in enumerate(
            (
                (update, update_out), (new_weights, weights_out),
                (new_first, first_out), (new_second, second_out),
            )
        )
    ]
    for copy in sent:
        copy.start()
    for q in range(4):
        places = [(place[0] + AWAY[2 * q + k]) % 8 * 256 for k in range(2)]
        chunks = [factor[pl.ds(pl.multiple_of(at, 256), 256)] for at in places]
        change[q % 2] = jnp.dot(
            jnp.concatenate(chunks), values, preferred_element_type=F32
        )
        for k in range(2):
            for at, block in blocks[2 * q + k]:
                rows = pl.ds(pl.multiple_of(at * 64, 64), 64)
                inner = pl.ds(pl.multiple_of(k * 256 + at % 4 * 64, 64), 64)
                for m in range(3):
                    before = block[m * 64 : (m + 1) * 64].astype(F32)
                    part = change[q % 2, inner, m * 128 : (m + 1) * 128]
                    copies[m, rows] = (before - 0.02 * part).astype(BF)
            rows = pl.ds(pl.multiple_of(places[k], 256), 256)
            for m in range(3):
                copy = pltpu.make_async_copy(
                    copies.at[m, rows], copies_out.at[m, rows], sems.at[2 * q + k, m]
                )
                copy.start()
                sent.append(copy)
    for copy in sent:
        copy.wait()


def step(inputs, cotangents, factor, weights, first_moment, second_moment):
    place = jnp.stack([lax.axis_index(axis) for axis in (Z, Y, CORE)]).astype(jnp.int32)
    smem = pl.BlockSpec(memory_space=pltpu.SMEM)
    hbm = pl.BlockSpec(memory_space=pl.ANY)
    half = pl.pallas_call(
        spread_kernel,
        out_shape=jax.ShapeDtypeStruct((8, 32, RANK), BF),
        in_specs=[smem, VMEM],
        out_specs=VMEM,
        compiler_params=pltpu.CompilerParams(vmem_limit_bytes=60 << 20),
    )(place, factor)
    half = lax.all_to_all(half, Z, split_axis=0, concat_axis=0, tiled=True)
    half = sent_to_all(half, Y)
    other_half = moved(half, CORE, 1)
    state = pl.pallas_call(
        state_kernel,
        out_shape=jax.ShapeDtypeStruct((1, 240, 128), BF),
        in_specs=[VMEM] * 3,
        out_specs=VMEM,
        compiler_params=pltpu.CompilerParams(vmem_limit_bytes=60 << 20),
    )(weights, first_moment, second_moment)
    state_z = gathered_z(state)
    states = gathered_y(state_z)


    gradient = (
        jnp.einsum("mtc,td->mcd", cotangents, inputs[:, :CUT], preferred_element_type=F32)
        .astype(BF)
        .reshape(384, CUT)
    )
    partial_value, factor_all = pl.pallas_call(
        partial_kernel,
        out_shape=(jax.ShapeDtypeStruct((32, 24, 128), BF), jax.ShapeDtypeStruct((2048, RANK), BF)),
        in_specs=[smem, VMEM, hbm, hbm, VMEM, VMEM],
        out_specs=(VMEM, hbm),
        scratch_shapes=[
            pltpu.VMEM((2048, RANK), BF),
            pltpu.VMEM((4, 512, 2048 - CUT), BF),
            pltpu.VMEM((3, 2048, 128), BF),
            pltpu.VMEM((384, 2048), BF),
            pltpu.VMEM((2048, RANK), BF),
            pltpu.SemaphoreType.DMA((7,)),
            pltpu.SemaphoreType.DMA,
        ],
        compiler_params=pltpu.CompilerParams(vmem_limit_bytes=50 << 20),
    )(place, gradient, cotangents, inputs, half, other_half)
    arrived = lax.all_to_all(partial_value, FS, split_axis=0, concat_axis=0, tiled=True)
    projected = arrived.astype(F32).sum(axis=0)
    projected_all = sent_to_all(projected.astype(BF), FS)
    squares = pl.pallas_call(
        square_kernel,
        out_shape=jax.ShapeDtypeStruct((8, 8, 128), F32),
        in_specs=[VMEM],
        out_specs=VMEM,
        compiler_params=pltpu.CompilerParams(vmem_limit_bytes=4 << 20),
    )(projected_all)
    squares = lax.all_to_all(squares, TP, split_axis=0, concat_axis=0, tiled=True)
    return pl.pallas_call(
        final_kernel,
        out_shape=(
            jax.ShapeDtypeStruct((3, 64, 128), F32),
            jax.ShapeDtypeStruct((3, 64, 128), F32),
            jax.ShapeDtypeStruct((3, 2048, 128), BF),
            jax.ShapeDtypeStruct((3, 8, 128), F32),
            jax.ShapeDtypeStruct((3, 8, 128), F32),
        ),
        in_specs=[smem] + [VMEM] * 13,
        out_specs=(hbm,) * 5,
        scratch_shapes=[
            pltpu.VMEM((3, 64, 128), F32),
            pltpu.VMEM((3, 64, 128), F32),
            pltpu.VMEM((3, 2048, 128), BF),
            pltpu.VMEM((3, 8, 128), F32),
            pltpu.VMEM((3, 8, 128), F32),
            pltpu.VMEM((RANK, 384), F32),
            pltpu.VMEM((2, 512, 384), F32),
            pltpu.SemaphoreType.DMA((4,)),
            pltpu.SemaphoreType.DMA((8, 3)),
        ],
        compiler_params=pltpu.CompilerParams(vmem_limit_bytes=24 << 20),
    )(
        place, squares, projected_all, projected, *states, first_moment, second_moment,
        weights, factor_all, factor,
    )


def solution(mesh):
    torus = Mesh(mesh.devices.reshape(8, 4, 4, 2), ("fs_0", "fs_1", "tp_0", "tp_1"))
    return jax.shard_map(
        step,
        mesh=torus,
        in_specs=(
            P(FS, None),
            P(None, FS, TP),
            P(FS, None),
            P(None, FS, TP),
            P(None, FS, TP),
            P(None, FS, TP),
        ),
        out_specs=(
            P(None, FS, TP),
            P(None, FS, TP),
            P(None, None, TP),
            P(None, FS, TP),
            P(None, FS, TP),
        ),
        check_vma=False,
    )
```

```python
import jax
import jax.numpy as jnp
from jax import lax
from jax.experimental import pallas as pl
from jax.experimental.pallas import tpu as pltpu
from jax.sharding import Mesh
from jax.sharding import PartitionSpec as P

MW = 1024
RANK = 256
Z, Y = ("fs_0", "fs_1")
FS = ("fs_0", "fs_1")
TP = ("tp_0", "tp_1")
CORE = "tp_1"
AWAY = (0, 7, 6, 5, 2, 1, 4, 3)
CUT = 1024
BF = jnp.bfloat16
F32 = jnp.float32
VMEM = pl.BlockSpec(memory_space=pltpu.VMEM)


def sent_to_all(array, axis):
    copies = jnp.broadcast_to(array, (lax.axis_size(axis), *array.shape))
    return lax.all_to_all(copies, axis, split_axis=0, concat_axis=0, tiled=True)


def moved(array, axis, shift):
    size = lax.axis_size(axis)
    return lax.ppermute(array, axis, [(i, (i + shift) % size) for i in range(size)])


def gathered_z(array):
    pair = jnp.concatenate([array, moved(array, Z, 1)])
    below = moved(pair, Z, 2)
    above = moved(pair, Z, -2)
    return jnp.concatenate([pair, below, above, moved(above, Z, -2)])


def gathered_y(array):
    right = moved(array, Y, 1)
    left = moved(array, Y, -1)
    return (
        array, right, left,
        moved(right[:4], Y, 1), moved(left[4:], Y, -1),
    )


def head_kernel(factor, weights, first, second, half, state):
    rows = factor[pl.ds(pl.multiple_of(lax.axis_index(CORE) * 32, 32), 32)]
    half[...] = jnp.broadcast_to(rows, half.shape)
    state[0, :192] = weights[...].reshape(192, 128).astype(BF)
    moments = jnp.concatenate([first[...].reshape(24, 128), second[...].reshape(24, 128)])
    state[0, 192:] = moments.astype(BF)


def partial_kernel(
    gradient_a, gradient_b, mine, other, out, factor_out, factor, held_a, held_b, sems
):
    copies = [
        pltpu.make_async_copy(gradient_a, held_a, sems.at[0]),
        pltpu.make_async_copy(gradient_b, held_b, sems.at[1]),
        pltpu.make_async_copy(factor, factor_out, sems.at[2]),
    ]
    copies[0].start()
    copies[1].start()
    first = lax.axis_index(CORE) * 32
    for z in range(8):
        for y in range(4):
            row = z * 256 + y * 64
            factor[pl.ds(row + pl.multiple_of(first, 32), 32)] = mine[y, z]
            factor[pl.ds(row + pl.multiple_of(32 - first, 32), 32)] = other[y, z]
    copies[2].start()
    copies[0].wait()
    projected = jnp.dot(held_a[...], factor[:CUT], preferred_element_type=F32)
    copies[1].wait()
    projected += jnp.dot(held_b[...], factor[CUT:], preferred_element_type=F32)
    rows = [projected[m * 128 : (m + 1) * 128].T.reshape(32, 8, 128) for m in range(3)]
    out[...] = jnp.concatenate(rows, axis=1).astype(BF)
    copies[2].wait()


def square_kernel(projected, out):
    values = projected[...].astype(F32).reshape(96, 8, 128)
    out[...] = jnp.broadcast_to(jnp.sum(values * values, axis=0), out.shape)


def moments(clip, projected, first, second):
    clipped = clip * projected
    new_first = 0.9 * first + 0.1 * clipped
    new_second = 0.95 * second + 0.05 * clipped * clipped
    return new_first, new_second, new_first / (jnp.sqrt(new_second) + 1e-08)


def final_kernel(
    squares, projected, own, state, right, left, across_a, across_b,
    first, second, weights, factor, own_factor,
    update_out, weights_out, copies_out, first_out, second_out,
    update, new_weights, copies, new_first, new_second, normed, change, own_sems, sems,
):
    place = (lax.axis_index(Z), lax.axis_index(Y))
    total = jnp.sum(jnp.sum(squares[...], axis=0), keepdims=True)
    root_mean = jnp.sqrt(total / (3 * RANK * MW) + 1e-06)
    clip = jnp.minimum(1.0, 0.25 / root_mean)

    def blocks_of(j):
        across = across_a.at[j] if j < 4 else across_b.at[j - 4]
        z = (place[0] + AWAY[j]) % 8
        return [
            (z * 4 + (place[1] + 4 - i) % 4, block)
            for i, block in enumerate((state.at[j], right.at[j], across, left.at[j]))
        ]

    blocks = [blocks_of(j) for j in range(8)]
    for m in range(3):
        own_first, own_second, _ = moments(
            clip, own[m * 8 : (m + 1) * 8], first[m], second[m]
        )
        new_first[m] = own_first
        new_second[m] = own_second
    for j in range(8):
        for at, block in blocks[j]:
            _, _, values = moments(
                clip,
                projected[at].astype(F32),
                block[192:216].astype(F32),
                block[216:240].astype(F32),
            )
            for m in range(3):
                normed[pl.ds(pl.multiple_of(at * 8, 8), 8), m * 128 : (m + 1) * 128] = values[
                    m * 8 : (m + 1) * 8
                ]
    values = normed[...].astype(BF)
    own_change = jnp.dot(own_factor[...], values, preferred_element_type=F32)
    for m in range(3):
        part = own_change[:, m * 128 : (m + 1) * 128]
        update[m] = part
        new_weights[m] = weights[m] - 0.02 * part
    sent = [
        pltpu.make_async_copy(source, target, own_sems.at[k])
        for k, (source, target) in enumerate(
            (
                (update, update_out), (new_weights, weights_out),
                (new_first, first_out), (new_second, second_out),
            )
        )
    ]
    for copy in sent:
        copy.start()
    for q in range(4):
        places = [(place[0] + AWAY[2 * q + k]) % 8 * 256 for k in range(2)]
        chunks = [factor[pl.ds(pl.multiple_of(at, 256), 256)] for at in places]
        change[q % 2] = jnp.dot(
            jnp.concatenate(chunks), values, preferred_element_type=F32
        )
        for k in range(2):
            for at, block in blocks[2 * q + k]:
                rows = pl.ds(pl.multiple_of(at * 64, 64), 64)
                inner = pl.ds(pl.multiple_of(k * 256 + at % 4 * 64, 64), 64)
                for m in range(3):
                    before = block[m * 64 : (m + 1) * 64].astype(F32)
                    part = change[q % 2, inner, m * 128 : (m + 1) * 128]
                    copies[m, rows] = (before - 0.02 * part).astype(BF)
            rows = pl.ds(pl.multiple_of(places[k], 256), 256)
            for m in range(3):
                copy = pltpu.make_async_copy(
                    copies.at[m, rows], copies_out.at[m, rows], sems.at[2 * q + k, m]
                )
                copy.start()
                sent.append(copy)
    for copy in sent:
        copy.wait()


def step(inputs, cotangents, factor, weights, first_moment, second_moment):
    hbm = pl.BlockSpec(memory_space=pl.ANY)
    half, state = pl.pallas_call(
        head_kernel,
        out_shape=(
            jax.ShapeDtypeStruct((8, 32, RANK), BF),
            jax.ShapeDtypeStruct((1, 240, 128), BF),
        ),
        in_specs=[VMEM] * 4,
        out_specs=(VMEM, VMEM),
        compiler_params=pltpu.CompilerParams(vmem_limit_bytes=60 << 20),
    )(factor, weights, first_moment, second_moment)
    half = lax.all_to_all(half, Z, split_axis=0, concat_axis=0, tiled=True)
    half = sent_to_all(half, Y)
    other_half = moved(half, CORE, 1)
    state_z = gathered_z(state)
    states = gathered_y(state_z)


    def gradient_of(part):
        return (
            jnp.einsum("mtc,td->mcd", cotangents, part, preferred_element_type=F32)
            .astype(BF)
            .reshape(384, -1)
        )

    gradient_a = gradient_of(inputs[:, :CUT])
    gradient_b = gradient_of(inputs[:, CUT:])
    partial_value, factor_all = pl.pallas_call(
        partial_kernel,
        out_shape=(
            jax.ShapeDtypeStruct((32, 24, 128), BF),
            jax.ShapeDtypeStruct((2048, RANK), BF),
        ),
        in_specs=[hbm, hbm, VMEM, VMEM],
        out_specs=(VMEM, hbm),
        scratch_shapes=[
            pltpu.VMEM((2048, RANK), BF),
            pltpu.VMEM((384, CUT), BF),
            pltpu.VMEM((384, 2048 - CUT), BF),
            pltpu.SemaphoreType.DMA((3,)),
        ],
        compiler_params=pltpu.CompilerParams(vmem_limit_bytes=60 << 20),
    )(gradient_a, gradient_b, half, other_half)
    arrived = lax.all_to_all(partial_value, FS, split_axis=0, concat_axis=0, tiled=True)
    projected = arrived.astype(F32).sum(axis=0)
    projected_all = sent_to_all(projected.astype(BF), FS)
    squares = pl.pallas_call(
        square_kernel,
        out_shape=jax.ShapeDtypeStruct((8, 8, 128), F32),
        in_specs=[VMEM],
        out_specs=VMEM,
        compiler_params=pltpu.CompilerParams(vmem_limit_bytes=4 << 20),
    )(projected_all)
    squares = lax.all_to_all(squares, TP, split_axis=0, concat_axis=0, tiled=True)
    return pl.pallas_call(
        final_kernel,
        out_shape=(
            jax.ShapeDtypeStruct((3, 64, 128), F32),
            jax.ShapeDtypeStruct((3, 64, 128), F32),
            jax.ShapeDtypeStruct((3, 2048, 128), BF),
            jax.ShapeDtypeStruct((3, 8, 128), F32),
            jax.ShapeDtypeStruct((3, 8, 128), F32),
        ),
        in_specs=[VMEM] * 13,
        out_specs=(hbm,) * 5,
        scratch_shapes=[
            pltpu.VMEM((3, 64, 128), F32),
            pltpu.VMEM((3, 64, 128), F32),
            pltpu.VMEM((3, 2048, 128), BF),
            pltpu.VMEM((3, 8, 128), F32),
            pltpu.VMEM((3, 8, 128), F32),
            pltpu.VMEM((RANK, 384), F32),
            pltpu.VMEM((2, 512, 384), F32),
            pltpu.SemaphoreType.DMA((4,)),
            pltpu.SemaphoreType.DMA((8, 3)),
        ],
        compiler_params=pltpu.CompilerParams(vmem_limit_bytes=24 << 20),
    )(
        squares, projected_all, projected, *states, first_moment, second_moment,
        weights, factor_all, factor,
    )


def solution(mesh):
    torus = Mesh(mesh.devices.reshape(8, 4, 4, 2), ("fs_0", "fs_1", "tp_0", "tp_1"))
    return jax.shard_map(
        step,
        mesh=torus,
        in_specs=(
            P(FS, None),
            P(None, FS, TP),
            P(FS, None),
            P(None, FS, TP),
            P(None, FS, TP),
            P(None, FS, TP),
        ),
        out_specs=(
            P(None, FS, TP),
            P(None, FS, TP),
            P(None, None, TP),
            P(None, FS, TP),
            P(None, FS, TP),
        ),
        check_vma=False,
    )
```

```python
import jax
import jax.numpy as jnp
from jax import lax
from jax.experimental import pallas as pl
from jax.experimental.pallas import tpu as pltpu
from jax.sharding import Mesh
from jax.sharding import PartitionSpec as P

MW = 1024
RANK = 256
Z, Y = ("fs_0", "fs_1")
FS = ("fs_0", "fs_1")
TP = ("tp_0", "tp_1")
CORE = "tp_1"
AWAY = (0, 4, 2, 6, 1, 5, 3, 7)
BF = jnp.bfloat16
F32 = jnp.float32
VMEM = pl.BlockSpec(memory_space=pltpu.VMEM)


def sent_to_all(array, axis):
    copies = jnp.broadcast_to(array, (lax.axis_size(axis), *array.shape))
    return lax.all_to_all(copies, axis, split_axis=0, concat_axis=0, tiled=True)


def moved(array, axis, shift):
    size = lax.axis_size(axis)
    return lax.ppermute(array, axis, [(i, (i + shift) % size) for i in range(size)])


def swapped(array, axis, bit):
    size = lax.axis_size(axis)
    return lax.ppermute(array, axis, [(i, i ^ bit) for i in range(size)])


def gathered_z(array):
    for bit in (4, 2, 1):
        array = jnp.concatenate([array, swapped(array, Z, bit)])
    return array


def gathered_y(array):
    right = moved(array, Y, 1)
    left = moved(array, Y, -1)
    return (
        array, right, left,
        moved(right[:4], Y, 1), moved(left[4:], Y, -1),
    )


def head_kernel(factor, weights, first, second, half, state):
    low, high = factor[:, :128], factor[:, 128:]
    columns = jnp.where(lax.axis_index(CORE) == 0, low, high)
    half[...] = jnp.broadcast_to(columns, half.shape)
    state[0, :192] = weights[...].reshape(192, 128).astype(BF)
    moments = jnp.concatenate([first[...].reshape(24, 128), second[...].reshape(24, 128)])
    state[0, 192:] = moments.astype(BF)


def partial_of(gradient, half):
    projected = jnp.dot(gradient[...], half[...].reshape(2048, 128), preferred_element_type=F32)
    rows = [projected[m * 128 : (m + 1) * 128].T.reshape(16, 8, 128) for m in range(3)]
    return jnp.concatenate(rows, axis=1).astype(BF)


def first_kernel(gradient, mine, out, mine_out, sem):
    copy = pltpu.make_async_copy(mine, mine_out, sem)
    copy.start()
    out[...] = partial_of(gradient, mine)
    copy.wait()


def second_kernel(gradient, other, before, out, other_out, sem):
    copy = pltpu.make_async_copy(other, other_out, sem)
    copy.start()
    first = lax.axis_index(CORE) * 16
    out[pl.ds(first, 16)] = before[...]
    out[pl.ds(16 - first, 16)] = partial_of(gradient, other)
    copy.wait()


def square_kernel(projected, out):
    values = projected[...].astype(F32).reshape(96, 8, 128)
    out[...] = jnp.broadcast_to(jnp.sum(values * values, axis=0), out.shape)


def moments(clip, projected, first, second):
    clipped = clip * projected
    new_first = 0.9 * first + 0.1 * clipped
    new_second = 0.95 * second + 0.05 * clipped * clipped
    return new_first, new_second, new_first / (jnp.sqrt(new_second) + 1e-08)


def final_kernel(
    squares, projected, own, state, right, left, across_a, across_b,
    first, second, weights, mine, other, own_factor,
    update_out, weights_out, copies_out, first_out, second_out,
    update, new_weights, copies, new_first, new_second, normed, change, own_sems, sems,
):
    place = (lax.axis_index(Z), lax.axis_index(Y))
    total = jnp.sum(jnp.sum(squares[...], axis=0), keepdims=True)
    root_mean = jnp.sqrt(total / (3 * RANK * MW) + 1e-06)
    clip = jnp.minimum(1.0, 0.25 / root_mean)

    def blocks_of(j):
        across = across_a.at[j] if j < 4 else across_b.at[j - 4]
        z = place[0] ^ AWAY[j]
        return [
            (z * 4 + (place[1] + 4 - i) % 4, block)
            for i, block in enumerate((state.at[j], right.at[j], across, left.at[j]))
        ]

    blocks = [blocks_of(j) for j in range(8)]
    for m in range(3):
        own_first, own_second, _ = moments(
            clip, own[m * 8 : (m + 1) * 8], first[m], second[m]
        )
        new_first[m] = own_first
        new_second[m] = own_second
    for j in range(8):
        for at, block in blocks[j]:
            _, _, values = moments(
                clip,
                projected[at].astype(F32),
                block[192:216].astype(F32),
                block[216:240].astype(F32),
            )
            for m in range(3):
                normed[pl.ds(pl.multiple_of(at * 8, 8), 8), m * 128 : (m + 1) * 128] = values[
                    m * 8 : (m + 1) * 8
                ]
    values = normed[...].astype(BF)
    side = lax.axis_index(CORE) * 128
    sided = jnp.concatenate(
        [normed[pl.ds(pl.multiple_of(at, 128), 128)] for at in (side, 128 - side)]
    ).astype(BF)
    own_change = jnp.dot(own_factor[...], values, preferred_element_type=F32)
    for m in range(3):
        part = own_change[:, m * 128 : (m + 1) * 128]
        update[m] = part
        new_weights[m] = weights[m] - 0.02 * part
    sent = [
        pltpu.make_async_copy(source, target, own_sems.at[k])
        for k, (source, target) in enumerate(
            (
                (update, update_out), (new_weights, weights_out),
                (new_first, first_out), (new_second, second_out),
            )
        )
    ]
    for copy in sent:
        copy.start()
    for q in range(4):
        places = [(place[0] ^ AWAY[2 * q + k]) * 256 for k in range(2)]
        chunks = [
            half[pl.ds(pl.multiple_of(at, 256), 256)] for half in (mine, other) for at in places
        ]
        change[q % 2] = jnp.dot(
            jnp.concatenate([jnp.concatenate(chunks[:2]), jnp.concatenate(chunks[2:])], axis=1),
            sided, preferred_element_type=F32,
        )
        for k in range(2):
            for at, block in blocks[2 * q + k]:
                rows = pl.ds(pl.multiple_of(at * 64, 64), 64)
                inner = pl.ds(pl.multiple_of(k * 256 + at % 4 * 64, 64), 64)
                for m in range(3):
                    before = block[m * 64 : (m + 1) * 64].astype(F32)
                    part = change[q % 2, inner, m * 128 : (m + 1) * 128]
                    copies[m, rows] = (before - 0.02 * part).astype(BF)
            rows = pl.ds(pl.multiple_of(places[k], 256), 256)
            for m in range(3):
                copy = pltpu.make_async_copy(
                    copies.at[m, rows], copies_out.at[m, rows], sems.at[2 * q + k, m]
                )
                copy.start()
                sent.append(copy)
    for copy in sent:
        copy.wait()


def step(inputs, cotangents, factor, weights, first_moment, second_moment):
    hbm = pl.BlockSpec(memory_space=pl.ANY)
    half, state = pl.pallas_call(
        head_kernel,
        out_shape=(
            jax.ShapeDtypeStruct((32, 64, 128), BF),
            jax.ShapeDtypeStruct((1, 240, 128), BF),
        ),
        in_specs=[VMEM] * 4,
        out_specs=(VMEM, VMEM),
        compiler_params=pltpu.CompilerParams(vmem_limit_bytes=60 << 20),
    )(factor, weights, first_moment, second_moment)
    half = lax.all_to_all(half, FS, split_axis=0, concat_axis=0, tiled=True)
    other_half = moved(half, CORE, 1)
    state_z = gathered_z(state)
    states = gathered_y(state_z)


    gradient = (
        jnp.einsum("mtc,td->mcd", cotangents, inputs, preferred_element_type=F32)
        .astype(BF)
        .reshape(384, 2048)
    )
    small = pltpu.CompilerParams(vmem_limit_bytes=8 << 20)
    half_shape = jax.ShapeDtypeStruct((32, 64, 128), BF)
    partial_first, mine = pl.pallas_call(
        first_kernel,
        out_shape=(jax.ShapeDtypeStruct((16, 24, 128), BF), half_shape),
        in_specs=[VMEM] * 2,
        out_specs=(VMEM, hbm),
        scratch_shapes=[pltpu.SemaphoreType.DMA],
        compiler_params=small,
    )(gradient, half)
    partial_value, other = pl.pallas_call(
        second_kernel,
        out_shape=(jax.ShapeDtypeStruct((32, 24, 128), BF), half_shape),
        in_specs=[VMEM] * 3,
        out_specs=(VMEM, hbm),
        scratch_shapes=[pltpu.SemaphoreType.DMA],
        compiler_params=small,
    )(gradient, other_half, partial_first)
    arrived = lax.all_to_all(partial_value, FS, split_axis=0, concat_axis=0, tiled=True)
    projected = arrived.astype(F32).sum(axis=0)
    projected_all = sent_to_all(projected.astype(BF), FS)
    squares = pl.pallas_call(
        square_kernel,
        out_shape=jax.ShapeDtypeStruct((8, 8, 128), F32),
        in_specs=[VMEM],
        out_specs=VMEM,
        compiler_params=pltpu.CompilerParams(vmem_limit_bytes=4 << 20),
    )(projected_all)
    squares = lax.all_to_all(squares, TP, split_axis=0, concat_axis=0, tiled=True)
    return pl.pallas_call(
        final_kernel,
        out_shape=(
            jax.ShapeDtypeStruct((3, 64, 128), F32),
            jax.ShapeDtypeStruct((3, 64, 128), F32),
            jax.ShapeDtypeStruct((3, 2048, 128), BF),
            jax.ShapeDtypeStruct((3, 8, 128), F32),
            jax.ShapeDtypeStruct((3, 8, 128), F32),
        ),
        in_specs=[VMEM] * 14,
        out_specs=(hbm,) * 5,
        scratch_shapes=[
            pltpu.VMEM((3, 64, 128), F32),
            pltpu.VMEM((3, 64, 128), F32),
            pltpu.VMEM((3, 2048, 128), BF),
            pltpu.VMEM((3, 8, 128), F32),
            pltpu.VMEM((3, 8, 128), F32),
            pltpu.VMEM((RANK, 384), F32),
            pltpu.VMEM((2, 512, 384), F32),
            pltpu.SemaphoreType.DMA((4,)),
            pltpu.SemaphoreType.DMA((8, 3)),
        ],
        compiler_params=pltpu.CompilerParams(vmem_limit_bytes=24 << 20),
    )(
        squares, projected_all, projected, *states, first_moment, second_moment,
        weights, mine.reshape(2048, 128), other.reshape(2048, 128), factor,
    )


def solution(mesh):
    torus = Mesh(mesh.devices.reshape(8, 4, 4, 2), ("fs_0", "fs_1", "tp_0", "tp_1"))
    return jax.shard_map(
        step,
        mesh=torus,
        in_specs=(
            P(FS, None),
            P(None, FS, TP),
            P(FS, None),
            P(None, FS, TP),
            P(None, FS, TP),
            P(None, FS, TP),
        ),
        out_specs=(
            P(None, FS, TP),
            P(None, FS, TP),
            P(None, None, TP),
            P(None, FS, TP),
            P(None, FS, TP),
        ),
        check_vma=False,
    )
```

```python
import jax
import jax.numpy as jnp
from jax import lax
from jax.experimental import pallas as pl
from jax.experimental.pallas import tpu as pltpu
from jax.sharding import Mesh
from jax.sharding import PartitionSpec as P

MW = 1024
RANK = 256
Z, Y = ("fs_0", "fs_1")
FS = ("fs_0", "fs_1")
TP = ("tp_0", "tp_1")
CORE = "tp_1"
AWAY = (0, 7, 2, 5, 1, 6, 3, 4)
CUT = 1024
BF = jnp.bfloat16
F32 = jnp.float32
VMEM = pl.BlockSpec(memory_space=pltpu.VMEM)


def sent_to_all(array, axis):
    copies = jnp.broadcast_to(array, (lax.axis_size(axis), *array.shape))
    return lax.all_to_all(copies, axis, split_axis=0, concat_axis=0, tiled=True)


def moved(array, axis, shift):
    size = lax.axis_size(axis)
    return lax.ppermute(array, axis, [(i, (i + shift) % size) for i in range(size)])


def swapped(array, axis, bit):
    size = lax.axis_size(axis)
    return lax.ppermute(array, axis, [(i, i ^ bit) for i in range(size)])


def gathered_z(array):
    for bit in (7, 2, 1):
        array = jnp.concatenate([array, swapped(array, Z, bit)])
    return array


def gathered_y(array):
    right = moved(array, Y, 1)
    left = moved(array, Y, -1)
    return (
        array, right, left,
        moved(right[:4], Y, 1), moved(left[4:], Y, -1),
    )


def head_kernel(factor, weights, first, second, half, state):
    low, high = factor[:, :128], factor[:, 128:]
    columns = jnp.where(lax.axis_index(CORE) == 0, low, high)
    half[...] = jnp.broadcast_to(columns, half.shape)
    state[0, :192] = weights[...].reshape(192, 128).astype(BF)
    moments = jnp.concatenate([first[...].reshape(24, 128), second[...].reshape(24, 128)])
    state[0, 192:] = moments.astype(BF)


def partial_of(gradient_a, gradient_b, half):
    rows = jnp.concatenate([half[:, z].reshape(256, 128) for z in range(8)])
    projected = jnp.dot(gradient_a[...], rows[:CUT], preferred_element_type=F32)
    projected += jnp.dot(gradient_b[...], rows[CUT:], preferred_element_type=F32)
    parts = [projected[m * 128 : (m + 1) * 128].T.reshape(16, 8, 128) for m in range(3)]
    return jnp.concatenate(parts, axis=1).astype(BF)


def first_kernel(gradient_a, gradient_b, mine, out, mine_out, sem):
    copy = pltpu.make_async_copy(mine, mine_out, sem)
    copy.start()
    out[...] = partial_of(gradient_a, gradient_b, mine)
    copy.wait()


def second_kernel(gradient_a, gradient_b, other, before, out, other_out, sem):
    copy = pltpu.make_async_copy(other, other_out, sem)
    copy.start()
    first = lax.axis_index(CORE) * 16
    out[pl.ds(first, 16)] = before[...]
    out[pl.ds(16 - first, 16)] = partial_of(gradient_a, gradient_b, other)
    copy.wait()


def square_kernel(projected, out):
    values = projected[...].astype(F32).reshape(96, 8, 128)
    out[...] = jnp.broadcast_to(jnp.sum(values * values, axis=0), out.shape)


def moments(clip, projected, first, second):
    clipped = clip * projected
    new_first = 0.9 * first + 0.1 * clipped
    new_second = 0.95 * second + 0.05 * clipped * clipped
    return new_first, new_second, new_first / (jnp.sqrt(new_second) + 1e-08)


def final_kernel(
    squares, projected, own, state, right, left, across_a, across_b,
    first, second, weights, mine, other, own_factor,
    update_out, weights_out, copies_out, first_out, second_out,
    update, new_weights, copies, new_first, new_second, normed, change, own_sems, sems,
):
    place = (lax.axis_index(Z), lax.axis_index(Y))
    total = jnp.sum(jnp.sum(squares[...], axis=0), keepdims=True)
    root_mean = jnp.sqrt(total / (3 * RANK * MW) + 1e-06)
    clip = jnp.minimum(1.0, 0.25 / root_mean)

    def blocks_of(j):
        across = across_a.at[j] if j < 4 else across_b.at[j - 4]
        z = place[0] ^ AWAY[j]
        return [
            (z * 4 + (place[1] + 4 - i) % 4, block)
            for i, block in enumerate((state.at[j], right.at[j], across, left.at[j]))
        ]

    blocks = [blocks_of(j) for j in range(8)]
    for m in range(3):
        own_first, own_second, _ = moments(
            clip, own[m * 8 : (m + 1) * 8], first[m], second[m]
        )
        new_first[m] = own_first
        new_second[m] = own_second
    for j in range(8):
        for at, block in blocks[j]:
            _, _, values = moments(
                clip,
                projected[at].astype(F32),
                block[192:216].astype(F32),
                block[216:240].astype(F32),
            )
            for m in range(3):
                normed[pl.ds(pl.multiple_of(at * 8, 8), 8), m * 128 : (m + 1) * 128] = values[
                    m * 8 : (m + 1) * 8
                ]
    values = normed[...].astype(BF)
    side = lax.axis_index(CORE) * 128
    sided = jnp.concatenate(
        [normed[pl.ds(pl.multiple_of(at, 128), 128)] for at in (side, 128 - side)]
    ).astype(BF)
    own_change = jnp.dot(own_factor[...], values, preferred_element_type=F32)
    for m in range(3):
        part = own_change[:, m * 128 : (m + 1) * 128]
        update[m] = part
        new_weights[m] = weights[m] - 0.02 * part
    sent = [
        pltpu.make_async_copy(source, target, own_sems.at[k])
        for k, (source, target) in enumerate(
            (
                (update, update_out), (new_weights, weights_out),
                (new_first, first_out), (new_second, second_out),
            )
        )
    ]
    for copy in sent:
        copy.start()
    for q in range(4):
        zs = [place[0] ^ AWAY[2 * q + k] for k in range(2)]
        sides = [
            jnp.concatenate([half[y, z] for z in zs for y in range(4)]) for half in (mine, other)
        ]
        change[q % 2] = jnp.dot(
            jnp.concatenate(sides, axis=1), sided, preferred_element_type=F32
        )
        for k in range(2):
            for at, block in blocks[2 * q + k]:
                rows = pl.ds(pl.multiple_of(at * 64, 64), 64)
                inner = pl.ds(pl.multiple_of(k * 256 + at % 4 * 64, 64), 64)
                for m in range(3):
                    before = block[m * 64 : (m + 1) * 64].astype(F32)
                    part = change[q % 2, inner, m * 128 : (m + 1) * 128]
                    copies[m, rows] = (before - 0.02 * part).astype(BF)
            rows = pl.ds(pl.multiple_of(zs[k] * 256, 256), 256)
            for m in range(3):
                copy = pltpu.make_async_copy(
                    copies.at[m, rows], copies_out.at[m, rows], sems.at[2 * q + k, m]
                )
                copy.start()
                sent.append(copy)
    for copy in sent:
        copy.wait()


def step(inputs, cotangents, factor, weights, first_moment, second_moment):
    hbm = pl.BlockSpec(memory_space=pl.ANY)
    half, state = pl.pallas_call(
        head_kernel,
        out_shape=(
            jax.ShapeDtypeStruct((8, 64, 128), BF),
            jax.ShapeDtypeStruct((1, 240, 128), BF),
        ),
        in_specs=[VMEM] * 4,
        out_specs=(VMEM, VMEM),
        compiler_params=pltpu.CompilerParams(vmem_limit_bytes=60 << 20),
    )(factor, weights, first_moment, second_moment)
    half = lax.all_to_all(half, Z, split_axis=0, concat_axis=0, tiled=True)
    half = sent_to_all(half, Y)
    other_half = moved(half, CORE, 1)
    state_z = gathered_z(state)
    states = gathered_y(state_z)


    def gradient_of(part):
        return (
            jnp.einsum("mtc,td->mcd", cotangents, part, preferred_element_type=F32)
            .astype(BF)
            .reshape(384, -1)
        )

    gradient_a = gradient_of(inputs[:, :CUT])
    gradient_b = gradient_of(inputs[:, CUT:])
    small = pltpu.CompilerParams(vmem_limit_bytes=8 << 20)
    half_shape = jax.ShapeDtypeStruct((4, 8, 64, 128), BF)
    partial_first, mine = pl.pallas_call(
        first_kernel,
        out_shape=(jax.ShapeDtypeStruct((16, 24, 128), BF), half_shape),
        in_specs=[VMEM] * 3,
        out_specs=(VMEM, hbm),
        scratch_shapes=[pltpu.SemaphoreType.DMA],
        compiler_params=small,
    )(gradient_a, gradient_b, half)
    partial_value, other = pl.pallas_call(
        second_kernel,
        out_shape=(jax.ShapeDtypeStruct((32, 24, 128), BF), half_shape),
        in_specs=[VMEM] * 4,
        out_specs=(VMEM, hbm),
        scratch_shapes=[pltpu.SemaphoreType.DMA],
        compiler_params=small,
    )(gradient_a, gradient_b, other_half, partial_first)
    arrived = lax.all_to_all(partial_value, FS, split_axis=0, concat_axis=0, tiled=True)
    projected = arrived.astype(F32).sum(axis=0)
    projected_all = sent_to_all(projected.astype(BF), FS)
    squares = pl.pallas_call(
        square_kernel,
        out_shape=jax.ShapeDtypeStruct((8, 8, 128), F32),
        in_specs=[VMEM],
        out_specs=VMEM,
        compiler_params=pltpu.CompilerParams(vmem_limit_bytes=4 << 20),
    )(projected_all)
    squares = lax.all_to_all(squares, TP, split_axis=0, concat_axis=0, tiled=True)
    return pl.pallas_call(
        final_kernel,
        out_shape=(
            jax.ShapeDtypeStruct((3, 64, 128), F32),
            jax.ShapeDtypeStruct((3, 64, 128), F32),
            jax.ShapeDtypeStruct((3, 2048, 128), BF),
            jax.ShapeDtypeStruct((3, 8, 128), F32),
            jax.ShapeDtypeStruct((3, 8, 128), F32),
        ),
        in_specs=[VMEM] * 14,
        out_specs=(hbm,) * 5,
        scratch_shapes=[
            pltpu.VMEM((3, 64, 128), F32),
            pltpu.VMEM((3, 64, 128), F32),
            pltpu.VMEM((3, 2048, 128), BF),
            pltpu.VMEM((3, 8, 128), F32),
            pltpu.VMEM((3, 8, 128), F32),
            pltpu.VMEM((RANK, 384), F32),
            pltpu.VMEM((2, 512, 384), F32),
            pltpu.SemaphoreType.DMA((4,)),
            pltpu.SemaphoreType.DMA((8, 3)),
        ],
        compiler_params=pltpu.CompilerParams(vmem_limit_bytes=24 << 20),
    )(
        squares, projected_all, projected, *states, first_moment, second_moment,
        weights, mine, other, factor,
    )


def solution(mesh):
    torus = Mesh(mesh.devices.reshape(8, 4, 4, 2), ("fs_0", "fs_1", "tp_0", "tp_1"))
    return jax.shard_map(
        step,
        mesh=torus,
        in_specs=(
            P(FS, None),
            P(None, FS, TP),
            P(FS, None),
            P(None, FS, TP),
            P(None, FS, TP),
            P(None, FS, TP),
        ),
        out_specs=(
            P(None, FS, TP),
            P(None, FS, TP),
            P(None, None, TP),
            P(None, FS, TP),
            P(None, FS, TP),
        ),
        check_vma=False,
    )
```

```python
import jax
import jax.numpy as jnp
from jax import lax
from jax.experimental import pallas as pl
from jax.experimental.pallas import tpu as pltpu
from jax.sharding import Mesh
from jax.sharding import PartitionSpec as P

MW = 1024
RANK = 256
Z, Y = ("fs_0", "fs_1")
FS = ("fs_0", "fs_1")
TP = ("tp_0", "tp_1")
CORE = "tp_1"
AWAY = (0, 7, 2, 5, 1, 6, 3, 4)
CUT = 1024
BF = jnp.bfloat16
F32 = jnp.float32
VMEM = pl.BlockSpec(memory_space=pltpu.VMEM)


def sent_to_all(array, axis):
    copies = jnp.broadcast_to(array, (lax.axis_size(axis), *array.shape))
    return lax.all_to_all(copies, axis, split_axis=0, concat_axis=0, tiled=True)


def moved(array, axis, shift):
    size = lax.axis_size(axis)
    return lax.ppermute(array, axis, [(i, (i + shift) % size) for i in range(size)])


def swapped(array, axis, bit):
    size = lax.axis_size(axis)
    return lax.ppermute(array, axis, [(i, i ^ bit) for i in range(size)])


def join_kernel(a, b, out):
    out[: a.shape[0]] = a[...]
    out[a.shape[0] :] = b[...]


def joined(a, b):
    return pl.pallas_call(
        join_kernel,
        out_shape=jax.ShapeDtypeStruct((2 * a.shape[0], *a.shape[1:]), a.dtype),
        in_specs=[VMEM] * 2,
        out_specs=VMEM,
        compiler_params=pltpu.CompilerParams(vmem_limit_bytes=4 << 20),
    )(a, b)


def gathered_z(array):
    for bit in (7, 2, 1):
        array = joined(array, swapped(array, Z, bit))
    return array


def gathered_y(array):
    right = moved(array, Y, 1)
    left = moved(array, Y, -1)
    return (
        array, right, left,
        moved(right[:4], Y, 1), moved(left[4:], Y, -1),
    )


def head_kernel(factor, weights, first, second, half, state):
    low, high = factor[:, :128], factor[:, 128:]
    columns = jnp.where(lax.axis_index(CORE) == 0, low, high)
    half[...] = jnp.broadcast_to(columns, half.shape)
    state[0, :192] = weights[...].reshape(192, 128).astype(BF)
    moments = jnp.concatenate([first[...].reshape(24, 128), second[...].reshape(24, 128)])
    state[0, 192:] = moments.astype(BF)


def partial_of(gradient_a, gradient_b, half):
    rows = jnp.concatenate([half[:, z].reshape(256, 128) for z in range(8)])
    projected = jnp.dot(gradient_a[...], rows[:CUT], preferred_element_type=F32)
    projected += jnp.dot(gradient_b[...], rows[CUT:], preferred_element_type=F32)
    parts = [projected[m * 128 : (m + 1) * 128].T.reshape(16, 8, 128) for m in range(3)]
    return jnp.concatenate(parts, axis=1).astype(BF)


def first_kernel(gradient_a, gradient_b, mine, out):
    out[...] = partial_of(gradient_a, gradient_b, mine)


def second_kernel(gradient_a, gradient_b, other, before, out):
    first = lax.axis_index(CORE) * 16
    out[pl.ds(first, 16)] = before[...]
    out[pl.ds(16 - first, 16)] = partial_of(gradient_a, gradient_b, other)


def square_kernel(projected, out):
    values = projected[...].astype(F32).reshape(96, 8, 128)
    out[...] = jnp.sum(values * values, axis=0)


def moments(clip, projected, first, second):
    clipped = clip * projected
    new_first = 0.9 * first + 0.1 * clipped
    new_second = 0.95 * second + 0.05 * clipped * clipped
    return new_first, new_second, new_first / (jnp.sqrt(new_second) + 1e-08)


def final_kernel(
    squares_0, squares_1, squares_2, squares_3, projected, own, state, right, left, across_a, across_b,
    first, second, weights, mine, other, own_factor,
    update_out, weights_out, copies_out, first_out, second_out,
    update, new_weights, copies, new_first, new_second, normed, change, own_sems, sems,
):
    place = (lax.axis_index(Z), lax.axis_index(Y))
    squares = (squares_0[...] + squares_1[...]) + (squares_2[...] + squares_3[...])
    total = jnp.sum(squares, keepdims=True)
    root_mean = jnp.sqrt(total / (3 * RANK * MW) + 1e-06)
    clip = jnp.minimum(1.0, 0.25 / root_mean)

    def blocks_of(j):
        across = across_a.at[j] if j < 4 else across_b.at[j - 4]
        z = place[0] ^ AWAY[j]
        return [
            (z * 4 + (place[1] + 4 - i) % 4, block)
            for i, block in enumerate((state.at[j], right.at[j], across, left.at[j]))
        ]

    blocks = [blocks_of(j) for j in range(8)]
    for m in range(3):
        own_first, own_second, _ = moments(
            clip, own[m * 8 : (m + 1) * 8], first[m], second[m]
        )
        new_first[m] = own_first
        new_second[m] = own_second
    for j in range(8):
        for at, block in blocks[j]:
            _, _, values = moments(
                clip,
                projected[at].astype(F32),
                block[192:216].astype(F32),
                block[216:240].astype(F32),
            )
            for m in range(3):
                normed[pl.ds(pl.multiple_of(at * 8, 8), 8), m * 128 : (m + 1) * 128] = values[
                    m * 8 : (m + 1) * 8
                ]
    values = normed[...].astype(BF)
    side = lax.axis_index(CORE) * 128
    sided = jnp.concatenate(
        [normed[pl.ds(pl.multiple_of(at, 128), 128)] for at in (side, 128 - side)]
    ).astype(BF)
    own_change = jnp.dot(own_factor[...], values, preferred_element_type=F32)
    for m in range(3):
        part = own_change[:, m * 128 : (m + 1) * 128]
        update[m] = part
        new_weights[m] = weights[m] - 0.02 * part
    sent = [
        pltpu.make_async_copy(source, target, own_sems.at[k])
        for k, (source, target) in enumerate(
            (
                (update, update_out), (new_weights, weights_out),
                (new_first, first_out), (new_second, second_out),
            )
        )
    ]
    for copy in sent:
        copy.start()
    for q in range(4):
        zs = [place[0] ^ AWAY[2 * q + k] for k in range(2)]
        sides = [
            jnp.concatenate([half[y, z] for z in zs for y in range(4)]) for half in (mine, other)
        ]
        change[q % 2] = jnp.dot(
            jnp.concatenate(sides, axis=1), sided, preferred_element_type=F32
        )
        for k in range(2):
            for at, block in blocks[2 * q + k]:
                rows = pl.ds(pl.multiple_of(at * 64, 64), 64)
                inner = pl.ds(pl.multiple_of(k * 256 + at % 4 * 64, 64), 64)
                for m in range(3):
                    before = block[m * 64 : (m + 1) * 64].astype(F32)
                    part = change[q % 2, inner, m * 128 : (m + 1) * 128]
                    copies[m, rows] = (before - 0.02 * part).astype(BF)
            rows = pl.ds(pl.multiple_of(zs[k] * 256, 256), 256)
            for m in range(3):
                copy = pltpu.make_async_copy(
                    copies.at[m, rows], copies_out.at[m, rows], sems.at[2 * q + k, m]
                )
                copy.start()
                sent.append(copy)
    for copy in sent:
        copy.wait()


def step(inputs, cotangents, factor, weights, first_moment, second_moment):
    hbm = pl.BlockSpec(memory_space=pl.ANY)
    half, state = pl.pallas_call(
        head_kernel,
        out_shape=(jax.ShapeDtypeStruct((8, 64, 128), BF), jax.ShapeDtypeStruct((1, 240, 128), BF)),
        in_specs=[VMEM] * 4,
        out_specs=(VMEM, VMEM),
        compiler_params=pltpu.CompilerParams(vmem_limit_bytes=60 << 20),
    )(factor, weights, first_moment, second_moment)
    half = lax.all_to_all(half, Z, split_axis=0, concat_axis=0, tiled=True)
    half = sent_to_all(half, Y)
    other_half = moved(half, CORE, 1)
    state_z = gathered_z(state)
    states = gathered_y(state_z)


    def gradient_of(part):
        return (
            jnp.einsum("mtc,td->mcd", cotangents, part, preferred_element_type=F32)
            .astype(BF)
            .reshape(384, -1)
        )

    gradient_a = gradient_of(inputs[:, :CUT])
    gradient_b = gradient_of(inputs[:, CUT:])
    small = pltpu.CompilerParams(vmem_limit_bytes=8 << 20)
    partial_first = pl.pallas_call(
        first_kernel,
        out_shape=jax.ShapeDtypeStruct((16, 24, 128), BF),
        in_specs=[VMEM] * 3,
        out_specs=VMEM,
        compiler_params=small,
    )(gradient_a, gradient_b, half)
    partial_value = pl.pallas_call(
        second_kernel,
        out_shape=jax.ShapeDtypeStruct((32, 24, 128), BF),
        in_specs=[VMEM] * 4,
        out_specs=VMEM,
        compiler_params=small,
    )(gradient_a, gradient_b, other_half, partial_first)
    arrived = lax.all_to_all(partial_value, FS, split_axis=0, concat_axis=0, tiled=True)
    projected = arrived.astype(F32).sum(axis=0)
    projected_all = sent_to_all(projected.astype(BF), FS)
    squares = pl.pallas_call(
        square_kernel,
        out_shape=jax.ShapeDtypeStruct((8, 128), F32),
        in_specs=[VMEM],
        out_specs=VMEM,
        compiler_params=pltpu.CompilerParams(vmem_limit_bytes=4 << 20),
    )(projected_all)
    squares += swapped(squares, CORE, 1)
    squares = [squares] + [swapped(squares, "tp_0", bit) for bit in (1, 2, 3)]
    return pl.pallas_call(
        final_kernel,
        out_shape=(
            jax.ShapeDtypeStruct((3, 64, 128), F32),
            jax.ShapeDtypeStruct((3, 64, 128), F32),
            jax.ShapeDtypeStruct((3, 2048, 128), BF),
            jax.ShapeDtypeStruct((3, 8, 128), F32),
            jax.ShapeDtypeStruct((3, 8, 128), F32),
        ),
        in_specs=[VMEM] * 17,
        out_specs=(hbm,) * 5,
        scratch_shapes=[
            pltpu.VMEM((3, 64, 128), F32),
            pltpu.VMEM((3, 64, 128), F32),
            pltpu.VMEM((3, 2048, 128), BF),
            pltpu.VMEM((3, 8, 128), F32),
            pltpu.VMEM((3, 8, 128), F32),
            pltpu.VMEM((RANK, 384), F32),
            pltpu.VMEM((2, 512, 384), F32),
            pltpu.SemaphoreType.DMA((4,)),
            pltpu.SemaphoreType.DMA((8, 3)),
        ],
        compiler_params=pltpu.CompilerParams(vmem_limit_bytes=24 << 20),
    )(
        *squares, projected_all, projected, *states, first_moment, second_moment,
        weights, half, other_half, factor,
    )


def solution(mesh):
    torus = Mesh(mesh.devices.reshape(8, 4, 4, 2), ("fs_0", "fs_1", "tp_0", "tp_1"))
    return jax.shard_map(
        step,
        mesh=torus,
        in_specs=(
            P(FS, None),
            P(None, FS, TP),
            P(FS, None),
            P(None, FS, TP),
            P(None, FS, TP),
            P(None, FS, TP),
        ),
        out_specs=(
            P(None, FS, TP),
            P(None, FS, TP),
            P(None, None, TP),
            P(None, FS, TP),
            P(None, FS, TP),
        ),
        check_vma=False,
    )
```

```python
import jax
import jax.numpy as jnp
from jax import lax
from jax.experimental import pallas as pl
from jax.experimental.pallas import tpu as pltpu
from jax.sharding import Mesh
from jax.sharding import PartitionSpec as P

MW = 1024
RANK = 256
Z, Y = ("fs_0", "fs_1")
FS = ("fs_0", "fs_1")
TP = ("tp_0", "tp_1")
CORE = "tp_1"
AWAY = (0, 7, 2, 5, 1, 6, 3, 4)
CUT = 1024
BF = jnp.bfloat16
F32 = jnp.float32
VMEM = pl.BlockSpec(memory_space=pltpu.VMEM)


def sent_to_all(array, axis):
    copies = jnp.broadcast_to(array, (lax.axis_size(axis), *array.shape))
    return lax.all_to_all(copies, axis, split_axis=0, concat_axis=0, tiled=True)


def moved(array, axis, shift):
    size = lax.axis_size(axis)
    return lax.ppermute(array, axis, [(i, (i + shift) % size) for i in range(size)])


def swapped(array, axis, bit):
    size = lax.axis_size(axis)
    return lax.ppermute(array, axis, [(i, i ^ bit) for i in range(size)])


def join_kernel(a, b, out):
    out[: a.shape[0]] = a[...]
    out[a.shape[0] :] = b[...]


def joined(a, b):
    return pl.pallas_call(
        join_kernel,
        out_shape=jax.ShapeDtypeStruct((2 * a.shape[0], *a.shape[1:]), a.dtype),
        in_specs=[VMEM] * 2,
        out_specs=VMEM,
        compiler_params=pltpu.CompilerParams(vmem_limit_bytes=4 << 20),
    )(a, b)


def gathered_z(array):
    for bit in (7, 2):
        array = joined(array, swapped(array, Z, bit))
    return array, swapped(array, Z, 1)


def gathered_y(a, b):
    right, left = moved(a, Y, 1), moved(b, Y, -1)
    other_right, other_left = moved(b, Y, 1), moved(a, Y, -1)
    across = moved(right, Y, 1), moved(left, Y, -1)
    return (a, right, across[0], other_left, b, other_right, across[1], left)


def head_kernel(factor, weights, first, second, half, state):
    low, high = factor[:, :128], factor[:, 128:]
    columns = jnp.where(lax.axis_index(CORE) == 0, low, high)
    half[...] = jnp.broadcast_to(columns, half.shape)
    state[0, :192] = weights[...].reshape(192, 128).astype(BF)
    moments = jnp.concatenate([first[...].reshape(24, 128), second[...].reshape(24, 128)])
    state[0, 192:] = moments.astype(BF)


def partial_of(gradient_a, gradient_b, half):
    rows = jnp.concatenate([half[:, z].reshape(256, 128) for z in range(8)])
    projected = jnp.dot(gradient_a[...], rows[:CUT], preferred_element_type=F32)
    projected += jnp.dot(gradient_b[...], rows[CUT:], preferred_element_type=F32)
    parts = [projected[m * 128 : (m + 1) * 128].T.reshape(16, 8, 128) for m in range(3)]
    return jnp.concatenate(parts, axis=1).astype(BF)


def first_kernel(gradient_a, gradient_b, mine, out):
    out[...] = partial_of(gradient_a, gradient_b, mine)


def second_kernel(gradient_a, gradient_b, other, before, out):
    first = lax.axis_index(CORE) * 16
    out[pl.ds(first, 16)] = before[...]
    out[pl.ds(16 - first, 16)] = partial_of(gradient_a, gradient_b, other)


def square_kernel(projected, out):
    values = projected[...].astype(F32).reshape(96, 8, 128)
    out[...] = jnp.sum(values * values, axis=0)


def moments(clip, projected, first, second):
    clipped = clip * projected
    new_first = 0.9 * first + 0.1 * clipped
    new_second = 0.95 * second + 0.05 * clipped * clipped
    return new_first, new_second, new_first / (jnp.sqrt(new_second) + 1e-08)


def final_kernel(
    squares_0, squares_1, squares_2, squares_3, projected, own,
    state_0, state_1, state_2, state_3, state_4, state_5, state_6, state_7,
    first, second, weights, mine, other,
    update_out, weights_out, copies_out, first_out, second_out,
    update, new_weights, copies, new_first, new_second, normed, change, held,
    own_sems, sems, held_sems,
):
    states = (state_0, state_1, state_2, state_3, state_4, state_5, state_6, state_7)
    brought = [
        [
            pltpu.make_async_copy(
                state.at[:, rows], held.at[k, :, rows], held_sems.at[k, part]
            )
            for k, state in enumerate(states)
        ]
        for part, rows in enumerate((pl.ds(192, 48), pl.ds(0, 192)))
    ]
    for copy in brought[0] + brought[1]:
        copy.start()
    place = (lax.axis_index(Z), lax.axis_index(Y))
    squares = (squares_0[...] + squares_1[...]) + (squares_2[...] + squares_3[...])
    total = jnp.sum(squares, keepdims=True)
    root_mean = jnp.sqrt(total / (3 * RANK * MW) + 1e-06)
    clip = jnp.minimum(1.0, 0.25 / root_mean)

    def blocks_of(j):
        z = place[0] ^ AWAY[j]
        return [
            (z * 4 + (place[1] + 4 - i) % 4, held.at[j // 4 * 4 + i, j % 4]) for i in range(4)
        ]

    blocks = [blocks_of(j) for j in range(8)]
    for m in range(3):
        own_first, own_second, _ = moments(
            clip, own[m * 8 : (m + 1) * 8], first[m], second[m]
        )
        new_first[m] = own_first
        new_second[m] = own_second
    for copy in brought[0]:
        copy.wait()
    for j in range(8):
        for at, block in blocks[j]:
            _, _, values = moments(
                clip,
                projected[at].astype(F32),
                block[192:216].astype(F32),
                block[216:240].astype(F32),
            )
            for m in range(3):
                normed[pl.ds(pl.multiple_of(at * 8, 8), 8), m * 128 : (m + 1) * 128] = values[
                    m * 8 : (m + 1) * 8
                ]
    side = lax.axis_index(CORE) * 128
    sided = jnp.concatenate(
        [normed[pl.ds(pl.multiple_of(at, 128), 128)] for at in (side, 128 - side)]
    ).astype(BF)
    own_rows = [half[place[1], place[0]] for half in (mine, other)]
    own_change = jnp.dot(
        jnp.concatenate(own_rows, axis=1), sided, preferred_element_type=F32
    )
    for m in range(3):
        part = own_change[:, m * 128 : (m + 1) * 128]
        update[m] = part
        new_weights[m] = weights[m] - 0.02 * part
    sent = [
        pltpu.make_async_copy(source, target, own_sems.at[k])
        for k, (source, target) in enumerate(
            (
                (update, update_out), (new_weights, weights_out),
                (new_first, first_out), (new_second, second_out),
            )
        )
    ]
    for copy in sent:
        copy.start()
    for copy in brought[1]:
        copy.wait()
    for q in range(4):
        zs = [place[0] ^ AWAY[2 * q + k] for k in range(2)]
        sides = [
            jnp.concatenate([half[y, z] for z in zs for y in range(4)]) for half in (mine, other)
        ]
        change[q % 2] = jnp.dot(
            jnp.concatenate(sides, axis=1), sided, preferred_element_type=F32
        )
        for k in range(2):
            for at, block in blocks[2 * q + k]:
                rows = pl.ds(pl.multiple_of(at * 64, 64), 64)
                inner = pl.ds(pl.multiple_of(k * 256 + at % 4 * 64, 64), 64)
                for m in range(3):
                    before = block[m * 64 : (m + 1) * 64].astype(F32)
                    part = change[q % 2, inner, m * 128 : (m + 1) * 128]
                    copies[m, rows] = (before - 0.02 * part).astype(BF)
            rows = pl.ds(pl.multiple_of(zs[k] * 256, 256), 256)
            for m in range(3):
                copy = pltpu.make_async_copy(
                    copies.at[m, rows], copies_out.at[m, rows], sems.at[2 * q + k, m]
                )
                copy.start()
                sent.append(copy)
    for copy in sent:
        copy.wait()


def step(inputs, cotangents, factor, weights, first_moment, second_moment):
    hbm = pl.BlockSpec(memory_space=pl.ANY)
    half, state = pl.pallas_call(
        head_kernel,
        out_shape=(jax.ShapeDtypeStruct((8, 64, 128), BF), jax.ShapeDtypeStruct((1, 240, 128), BF)),
        in_specs=[VMEM] * 4,
        out_specs=(VMEM, VMEM),
        compiler_params=pltpu.CompilerParams(vmem_limit_bytes=60 << 20),
    )(factor, weights, first_moment, second_moment)
    half = lax.all_to_all(half, Z, split_axis=0, concat_axis=0, tiled=True)
    half = sent_to_all(half, Y)
    other_half = moved(half, CORE, 1)
    states = gathered_y(*gathered_z(state))


    def gradient_of(part):
        return (
            jnp.einsum("mtc,td->mcd", cotangents, part, preferred_element_type=F32)
            .astype(BF)
            .reshape(384, -1)
        )

    gradient_a = gradient_of(inputs[:, :CUT])
    gradient_b = gradient_of(inputs[:, CUT:])
    small = pltpu.CompilerParams(vmem_limit_bytes=8 << 20)
    partial_first = pl.pallas_call(
        first_kernel,
        out_shape=jax.ShapeDtypeStruct((16, 24, 128), BF),
        in_specs=[VMEM] * 3,
        out_specs=VMEM,
        compiler_params=small,
    )(gradient_a, gradient_b, half)
    partial_value = pl.pallas_call(
        second_kernel,
        out_shape=jax.ShapeDtypeStruct((32, 24, 128), BF),
        in_specs=[VMEM] * 4,
        out_specs=VMEM,
        compiler_params=small,
    )(gradient_a, gradient_b, other_half, partial_first)
    arrived = lax.all_to_all(partial_value, FS, split_axis=0, concat_axis=0, tiled=True)
    projected = arrived.astype(F32).sum(axis=0)
    projected_all = sent_to_all(projected.astype(BF), FS)
    squares = pl.pallas_call(
        square_kernel,
        out_shape=jax.ShapeDtypeStruct((8, 128), F32),
        in_specs=[VMEM],
        out_specs=VMEM,
        compiler_params=pltpu.CompilerParams(vmem_limit_bytes=4 << 20),
    )(projected_all)
    squares += swapped(squares, CORE, 1)
    squares = [squares] + [swapped(squares, "tp_0", bit) for bit in (1, 2, 3)]
    return pl.pallas_call(
        final_kernel,
        out_shape=(
            jax.ShapeDtypeStruct((3, 64, 128), F32),
            jax.ShapeDtypeStruct((3, 64, 128), F32),
            jax.ShapeDtypeStruct((3, 2048, 128), BF),
            jax.ShapeDtypeStruct((3, 8, 128), F32),
            jax.ShapeDtypeStruct((3, 8, 128), F32),
        ),
        in_specs=[VMEM] * 6 + [hbm] * 8 + [VMEM] * 5,
        out_specs=(hbm,) * 5,
        scratch_shapes=[
            pltpu.VMEM((3, 64, 128), F32),
            pltpu.VMEM((3, 64, 128), F32),
            pltpu.VMEM((3, 2048, 128), BF),
            pltpu.VMEM((3, 8, 128), F32),
            pltpu.VMEM((3, 8, 128), F32),
            pltpu.VMEM((RANK, 384), F32),
            pltpu.VMEM((2, 512, 384), F32),
            pltpu.VMEM((8, 4, 240, 128), BF),
            pltpu.SemaphoreType.DMA((4,)),
            pltpu.SemaphoreType.DMA((8, 3)),
            pltpu.SemaphoreType.DMA((8, 2)),
        ],
        compiler_params=pltpu.CompilerParams(vmem_limit_bytes=24 << 20),
    )(
        *squares, projected_all, projected, *states, first_moment, second_moment,
        weights, half, other_half,
    )


def solution(mesh):
    torus = Mesh(mesh.devices.reshape(8, 4, 4, 2), ("fs_0", "fs_1", "tp_0", "tp_1"))
    return jax.shard_map(
        step,
        mesh=torus,
        in_specs=(
            P(FS, None),
            P(None, FS, TP),
            P(FS, None),
            P(None, FS, TP),
            P(None, FS, TP),
            P(None, FS, TP),
        ),
        out_specs=(
            P(None, FS, TP),
            P(None, FS, TP),
            P(None, None, TP),
            P(None, FS, TP),
            P(None, FS, TP),
        ),
        check_vma=False,
    )
```

```python
import jax
import jax.numpy as jnp
from jax import lax
from jax.experimental import pallas as pl
from jax.experimental.pallas import tpu as pltpu
from jax.sharding import Mesh
from jax.sharding import PartitionSpec as P

MW = 1024
RANK = 256
Z, Y = ("fs_0", "fs_1")
FS = ("fs_0", "fs_1")
TP = ("tp_0", "tp_1")
CORE = "tp_1"
AWAY = (0, 7, 2, 5, 1, 6, 3, 4)
CUT = 1024
BF = jnp.bfloat16
F32 = jnp.float32
VMEM = pl.BlockSpec(memory_space=pltpu.VMEM)


def sent_to_all(array, axis):
    copies = jnp.broadcast_to(array, (lax.axis_size(axis), *array.shape))
    return lax.all_to_all(copies, axis, split_axis=0, concat_axis=0, tiled=True)


def moved(array, axis, shift):
    size = lax.axis_size(axis)
    return lax.ppermute(array, axis, [(i, (i + shift) % size) for i in range(size)])


def swapped(array, axis, bit):
    size = lax.axis_size(axis)
    return lax.ppermute(array, axis, [(i, i ^ bit) for i in range(size)])


def join_kernel(a, b, out):
    out[: a.shape[0]] = a[...]
    out[a.shape[0] :] = b[...]


def joined(a, b):
    return pl.pallas_call(
        join_kernel,
        out_shape=jax.ShapeDtypeStruct((2 * a.shape[0], *a.shape[1:]), a.dtype),
        in_specs=[VMEM] * 2,
        out_specs=VMEM,
        compiler_params=pltpu.CompilerParams(vmem_limit_bytes=60 << 20),
    )(a, b)


def gathered_z(array):
    for bit in (7, 2):
        array = joined(array, swapped(array, Z, bit))
    return array, swapped(array, Z, 1)


def gathered_y(a, b):
    right, left = moved(a, Y, 1), moved(b, Y, -1)
    other_right, other_left = moved(b, Y, 1), moved(a, Y, -1)
    across = moved(right, Y, 1), moved(left, Y, -1)
    return (a, right, across[0], other_left, b, other_right, across[1], left)


def head_kernel(factor, weights, first, second, half, state):
    low, high = factor[:, :128], factor[:, 128:]
    columns = jnp.where(lax.axis_index(CORE) == 0, low, high)
    half[...] = jnp.broadcast_to(columns, half.shape)
    state[0, :192] = weights[...].reshape(192, 128).astype(BF)
    moments = jnp.concatenate([first[...].reshape(24, 128), second[...].reshape(24, 128)])
    state[0, 192:] = moments.astype(BF)


def partial_of(gradient_a, gradient_b, half):
    rows = jnp.concatenate([half[:, z].reshape(256, 128) for z in range(8)])
    projected = jnp.dot(gradient_a[...], rows[:CUT], preferred_element_type=F32)
    projected += jnp.dot(gradient_b[...], rows[CUT:], preferred_element_type=F32)
    parts = [projected[m * 128 : (m + 1) * 128].T.reshape(16, 8, 128) for m in range(3)]
    return jnp.concatenate(parts, axis=1).astype(BF)


def first_kernel(gradient_a, gradient_b, mine, out):
    out[...] = partial_of(gradient_a, gradient_b, mine)


def second_kernel(gradient_a, gradient_b, other, before, out):
    first = lax.axis_index(CORE) * 16
    out[pl.ds(first, 16)] = before[...]
    out[pl.ds(16 - first, 16)] = partial_of(gradient_a, gradient_b, other)


def square_kernel(projected, out):
    values = projected[...].astype(F32).reshape(96, 8, 128)
    out[...] = jnp.sum(values * values, axis=0)


def moments(clip, projected, first, second):
    clipped = clip * projected
    new_first = 0.9 * first + 0.1 * clipped
    new_second = 0.95 * second + 0.05 * clipped * clipped
    return new_first, new_second, new_first / (jnp.sqrt(new_second) + 1e-08)


def final_kernel(
    squares_0, squares_1, projected, own,
    state_0, state_1, state_2, state_3, state_4, state_5, state_6, state_7,
    first, second, weights, mine, other,
    update_out, weights_out, copies_out, first_out, second_out,
    update, new_weights, copies, new_first, new_second, normed, change, held,
    own_sems, sems, held_sems,
):
    states = (state_0, state_1, state_2, state_3, state_4, state_5, state_6, state_7)
    brought = [
        [
            pltpu.make_async_copy(
                state.at[:, rows], held.at[k, :, rows], held_sems.at[k, part]
            )
            for k, state in enumerate(states)
        ]
        for part, rows in enumerate((pl.ds(192, 48), pl.ds(0, 192)))
    ]
    for copy in brought[0] + brought[1]:
        copy.start()
    place = (lax.axis_index(Z), lax.axis_index(Y))
    total = jnp.sum(squares_0[...] + squares_1[...], keepdims=True)
    root_mean = jnp.sqrt(total / (3 * RANK * MW) + 1e-06)
    clip = jnp.minimum(1.0, 0.25 / root_mean)

    def blocks_of(j):
        z = place[0] ^ AWAY[j]
        return [
            (z * 4 + (place[1] + 4 - i) % 4, held.at[j // 4 * 4 + i, j % 4]) for i in range(4)
        ]

    blocks = [blocks_of(j) for j in range(8)]
    for m in range(3):
        own_first, own_second, _ = moments(
            clip, own[m * 8 : (m + 1) * 8], first[m], second[m]
        )
        new_first[m] = own_first
        new_second[m] = own_second
    for copy in brought[0]:
        copy.wait()
    for j in range(8):
        for at, block in blocks[j]:
            _, _, values = moments(
                clip,
                projected[at].astype(F32),
                block[192:216].astype(F32),
                block[216:240].astype(F32),
            )
            for m in range(3):
                normed[pl.ds(pl.multiple_of(at * 8, 8), 8), m * 128 : (m + 1) * 128] = values[
                    m * 8 : (m + 1) * 8
                ]
    side = lax.axis_index(CORE) * 128
    sided = jnp.concatenate(
        [normed[pl.ds(pl.multiple_of(at, 128), 128)] for at in (side, 128 - side)]
    ).astype(BF)
    own_rows = [half[place[1], place[0]] for half in (mine, other)]
    own_change = jnp.dot(
        jnp.concatenate(own_rows, axis=1), sided, preferred_element_type=F32
    )
    for m in range(3):
        part = own_change[:, m * 128 : (m + 1) * 128]
        update[m] = part
        new_weights[m] = weights[m] - 0.02 * part
    sent = [
        pltpu.make_async_copy(source, target, own_sems.at[k])
        for k, (source, target) in enumerate(
            (
                (update, update_out), (new_weights, weights_out),
                (new_first, first_out), (new_second, second_out),
            )
        )
    ]
    for copy in sent:
        copy.start()
    for copy in brought[1]:
        copy.wait()
    for q in range(4):
        zs = [place[0] ^ AWAY[2 * q + k] for k in range(2)]
        sides = [
            jnp.concatenate([half[y, z] for z in zs for y in range(4)]) for half in (mine, other)
        ]
        change[q % 2] = jnp.dot(
            jnp.concatenate(sides, axis=1), sided, preferred_element_type=F32
        )
        for k in range(2):
            for at, block in blocks[2 * q + k]:
                rows = pl.ds(pl.multiple_of(at * 64, 64), 64)
                inner = pl.ds(pl.multiple_of(k * 256 + at % 4 * 64, 64), 64)
                for m in range(3):
                    before = block[m * 64 : (m + 1) * 64].astype(F32)
                    part = change[q % 2, inner, m * 128 : (m + 1) * 128]
                    copies[m, rows] = (before - 0.02 * part).astype(BF)
            rows = pl.ds(pl.multiple_of(zs[k] * 256, 256), 256)
            for m in range(3):
                copy = pltpu.make_async_copy(
                    copies.at[m, rows], copies_out.at[m, rows], sems.at[2 * q + k, m]
                )
                copy.start()
                sent.append(copy)
    for copy in sent:
        copy.wait()


def step(inputs, cotangents, factor, weights, first_moment, second_moment):
    hbm = pl.BlockSpec(memory_space=pl.ANY)
    half, state = pl.pallas_call(
        head_kernel,
        out_shape=(
            jax.ShapeDtypeStruct((8, 64, 128), BF),
            jax.ShapeDtypeStruct((1, 240, 128), BF),
        ),
        in_specs=[VMEM] * 4,
        out_specs=(VMEM, VMEM),
        compiler_params=pltpu.CompilerParams(vmem_limit_bytes=60 << 20),
    )(factor, weights, first_moment, second_moment)
    half = lax.all_to_all(half, Z, split_axis=0, concat_axis=0, tiled=True)
    half = sent_to_all(half, Y)
    other_half = moved(half, CORE, 1)
    states = gathered_y(*gathered_z(state))


    def gradient_of(part):
        return (
            jnp.einsum("mtc,td->mcd", cotangents, part, preferred_element_type=F32)
            .astype(BF)
            .reshape(384, -1)
        )

    gradient_a = gradient_of(inputs[:, :CUT])
    gradient_b = gradient_of(inputs[:, CUT:])
    small = pltpu.CompilerParams(vmem_limit_bytes=8 << 20)
    partial_first = pl.pallas_call(
        first_kernel,
        out_shape=jax.ShapeDtypeStruct((16, 24, 128), BF),
        in_specs=[VMEM] * 3,
        out_specs=VMEM,
        compiler_params=small,
    )(gradient_a, gradient_b, half)
    partial_value = pl.pallas_call(
        second_kernel,
        out_shape=jax.ShapeDtypeStruct((32, 24, 128), BF),
        in_specs=[VMEM] * 4,
        out_specs=VMEM,
        compiler_params=small,
    )(gradient_a, gradient_b, other_half, partial_first)
    arrived = lax.all_to_all(partial_value, FS, split_axis=0, concat_axis=0, tiled=True)
    projected = arrived.astype(F32).sum(axis=0)
    projected_all = sent_to_all(projected.astype(BF), FS)
    squares = pl.pallas_call(
        square_kernel,
        out_shape=jax.ShapeDtypeStruct((8, 128), F32),
        in_specs=[VMEM],
        out_specs=VMEM,
        compiler_params=pltpu.CompilerParams(vmem_limit_bytes=4 << 20),
    )(projected_all)
    squares += swapped(squares, CORE, 1)
    squares += swapped(squares, "tp_0", 1)
    squares = (squares, swapped(squares, "tp_0", 3))
    return pl.pallas_call(
        final_kernel,
        out_shape=(
            jax.ShapeDtypeStruct((3, 64, 128), F32),
            jax.ShapeDtypeStruct((3, 64, 128), F32),
            jax.ShapeDtypeStruct((3, 2048, 128), BF),
            jax.ShapeDtypeStruct((3, 8, 128), F32),
            jax.ShapeDtypeStruct((3, 8, 128), F32),
        ),
        in_specs=[VMEM] * 4 + [hbm] * 8 + [VMEM] * 5,
        out_specs=(hbm,) * 5,
        scratch_shapes=[
            pltpu.VMEM((3, 64, 128), F32),
            pltpu.VMEM((3, 64, 128), F32),
            pltpu.VMEM((3, 2048, 128), BF),
            pltpu.VMEM((3, 8, 128), F32),
            pltpu.VMEM((3, 8, 128), F32),
            pltpu.VMEM((RANK, 384), F32),
            pltpu.VMEM((2, 512, 384), F32),
            pltpu.VMEM((8, 4, 240, 128), BF),
            pltpu.SemaphoreType.DMA((4,)),
            pltpu.SemaphoreType.DMA((8, 3)),
            pltpu.SemaphoreType.DMA((8, 2)),
        ],
        compiler_params=pltpu.CompilerParams(vmem_limit_bytes=24 << 20),
    )(
        *squares, projected_all, projected, *states, first_moment, second_moment,
        weights, half, other_half,
    )


def solution(mesh):
    torus = Mesh(mesh.devices.reshape(8, 4, 4, 2), ("fs_0", "fs_1", "tp_0", "tp_1"))
    return jax.shard_map(
        step,
        mesh=torus,
        in_specs=(
            P(FS, None),
            P(None, FS, TP),
            P(FS, None),
            P(None, FS, TP),
            P(None, FS, TP),
            P(None, FS, TP),
        ),
        out_specs=(
            P(None, FS, TP),
            P(None, FS, TP),
            P(None, None, TP),
            P(None, FS, TP),
            P(None, FS, TP),
        ),
        check_vma=False,
    )
```
